32 devices in a mesh: st: 8 (over z, y), tp: 4 (over x, core).
Axes of the slice: x: 2, y: 2, z: 4, core: 2. Of those that a mesh axis runs over, the one named last changes fastest.
Arguments:
- queries: bfloat16 [8192, 1024], P('st', 'tp'), may hold values from -540 to 540
- gate_pre: bfloat16 [8192, 1024], P('st', 'tp'), may hold values from -6 to 6
- cotangent: bfloat16 [8192, 1024], P('st', 'tp'), may hold values from -6 to 6
- store: bfloat16 [10240, 2048], P('st'), may hold values from -6 to 6
- store_gain: float32 [2048], replicated, may hold values from 0.1 to 1.9
- w_key: bfloat16 [2048, 1024], P(None, 'tp'), may hold values from -0.125 to 0.125
- w_value: bfloat16 [2048, 1024], P(None, 'tp'), may hold values from -0.125 to 0.125
- owners: int32 [64, 4], P('st'), may hold values from 0 to 7, all different within a row; in each aligned block of 8 rows (0 to 7, 8 to 15, ...) at most 8 rows name the same one
- slots: int32 [64, 4], P('st'), may hold values from 0 to 19
Outputs:
- grad_queries: float32 [8192, 1024], P('st', 'tp')
- grad_store: float32 [10240, 2048], P(('st', 'tp'))
- grad_w_value: float32 [2048, 1024], P('st', 'tp')
The draws below stay inside these ranges and needn't reach their ends.
Inputs may be any that keep to these rules, and one draw needn't show every extreme that they name: Each block names 4 different owners. Among the blocks of one device no owner is named twice.
All inputs are finite; a program needn't handle non-finite values.
Results may differ from the reference program's by a relative error of at most 0.014.
Values may be sent and summed in bfloat16 or wider, within the bound.
A program may use at most 192 MiB of HBM per device.

```python
import math
import jax
import jax.numpy as jnp
import numpy as np
from jax import lax

D = 2048
HEADS = 8
HD = 128
PLEN = 64
BLK = 128
NPB = 4
PASS_DEV = 20
XW = 1024
BLK_DEV = 8
CAP = 8
TOKENS = 8192
BLOCKS = 64
PASSAGES = 160
ROWS = 10240
N_ST = 8


def draw_queries(key, part):
    first_key = jax.random.fold_in(key, 11)
    drawn = jnp.clip(jax.random.normal(first_key, (TOKENS, XW), jnp.float32), -6.0, 6.0)
    return drawn.astype(jnp.bfloat16)


def draw_cotangent(key, part):
    first_key = jax.random.fold_in(key, 13)
    drawn = jnp.clip(jax.random.normal(first_key, (TOKENS, XW), jnp.float32), -6.0, 6.0)
    return drawn.astype(jnp.bfloat16)


def set_ends(array, stream_key, least, high):
    place = [jax.random.randint(jax.random.fold_in(stream_key, axis), (), 0, length) for axis, length in enumerate(array.shape)]
    widest = array.shape.index(max(array.shape))
    neighbour = place[:widest] + [(place[widest] + 1) % array.shape[widest]] + place[widest + 1:]
    return array.at[tuple(place)].set(least).at[tuple(neighbour)].set(high)


def shard_levels(key, extent, shards, low, largest):
    gain = 1.0
    for position, shards_of in shards:
        heights = jax.random.uniform(jax.random.fold_in(jax.random.fold_in(key, 6), position), (shards_of,), jnp.float32, low / len(shards), largest / len(shards))
        gain = gain * jnp.repeat(jnp.exp(heights), extent[position] // shards_of).reshape((-1,) + (1,) * (len(extent) - 1 - position))
    return gain


def rank_bounds(number_of, skew):
    portions = [(1 << 20) // math.isqrt(grade ** skew) + 1 for grade in range(1, number_of + 1)]
    width = 1 + sum(portions) // (1 << 30)
    return np.cumsum(np.array([max(1, weight // width) for weight in portions]))


def ranked_ids(rng, dims, count, skew):
    table = rank_bounds(count, skew)
    lot = jax.random.randint(jax.random.fold_in(rng, 1), dims, 0, int(table[count - 1]))
    standing = jnp.searchsorted(jnp.asarray(table, jnp.int32), lot, side="right")
    return jax.random.permutation(jax.random.fold_in(rng, 2), count)[standing].astype(jnp.int32)


def routed_block(own_key, own, number, rows, count, top, bound, lean):
    sequence = jax.random.permutation(own_key, count)
    heavy_load, common = portions_of(count, rows * top, bound, lean, True), portions_of(count, rows * top, bound, lean, False)
    places = jnp.arange(count)

    def named(lengths, rotation):
        used = int((lengths > 0).sum())
        fixed = max(1, used // 4)
        moved = fixed + (places - fixed + rotation * (used - fixed)) % max(1, count - fixed)
        return jnp.zeros((count,), jnp.int32).at[sequence[jnp.where(places < fixed, places, moved)]].set(jnp.asarray(lengths, jnp.int32))

    lengths = jnp.where(number % 4 == 0, named(heavy_load, number // 4), named(common, number - number // 4 - 1))
    mixed = jax.random.permutation(jax.random.fold_in(own, 3), count)
    giver, sink = mixed[0:count // 2 * 2:2], mixed[1:count // 2 * 2:2]
    room = jnp.minimum(lengths[giver] - 1, bound - lengths[sink]) // 2
    room = jnp.where((giver == sequence[0]) | (sink == sequence[0]) | (lengths[sink] == 0), 0, jnp.maximum(room, 0))
    moved = jax.random.randint(jax.random.fold_in(own, 4), (count // 2,), 0, 1 << 20) % (room + 1)
    lengths = lengths.at[giver].add(-moved).at[sink].add(moved)
    labels = jnp.searchsorted(jnp.cumsum(lengths), jnp.arange(rows * top), side="right").astype(jnp.int32)
    listing = labels.reshape(top, rows).T
    listing = listing[jax.random.permutation(jax.random.fold_in(own, 1), rows)]
    rotation = jax.random.randint(jax.random.fold_in(own, 2), (rows, 1), 0, top)
    return jnp.take_along_axis(listing, (jnp.arange(top)[None, :] + rotation) % top, axis=1)


def portions_of(amount, total, bound, slope, full):
    weights = [(1 << 20) // math.isqrt(rank ** slope) + 1 for rank in range(1, amount + 1)]
    largest = bound if full else min(bound, max(-(-total // amount), total * weights[0] // sum(weights)))
    least = 1 if total - largest >= amount - 1 else 0
    counts, surplus = [largest] + [least] * (amount - 1), total - largest - least * (amount - 1)
    while surplus > 0:
        movable = [i for i in range(1, amount) if counts[i] < largest] or [i for i in range(1, amount) if counts[i] < bound]
        whole, budget = sum([weights[i] for i in movable]), surplus
        for i in movable:
            addition = min(bound - counts[i], max(1, budget * weights[i] // whole), surplus)
            counts[i] = counts[i] + addition
            surplus = surplus - addition
    return np.array(counts)


def normal_values(own_key, dims, scale, bound, split=(), kind=jnp.bfloat16):
    factor_of = shard_levels(own_key, dims, split, -0.22, 0.18) if split else 1.0
    values = jax.random.normal(own_key, dims, jnp.float32) * scale * factor_of
    return jnp.minimum(jnp.maximum(values, -bound), bound).astype(kind)


def setup_inputs(seed: int = 0) -> dict:
    key_of = jax.random.split(jax.random.key(seed), 10)
    queries = draw_queries(jax.random.fold_in(key_of[9], 71), 0)
    gate_pre = normal_values(key_of[1], (TOKENS, XW), 1.5, 6.0, ((0, 8), (1, 4)))
    cotangent = draw_cotangent(jax.random.fold_in(key_of[9], 71), 0)
    store = normal_values(key_of[3], (ROWS, D), 1.0, 6.0, ((0, 8),))
    store_gain = jnp.clip(1.0 + 0.18 * jax.random.normal(key_of[4], (D,), jnp.float32), 0.1, 1.9)
    w_key = normal_values(key_of[5], (D, XW), D ** -0.5, 0.125, ((1, 4),))
    w_value = normal_values(key_of[6], (D, XW), D ** -0.5, 0.125, ((1, 4),))
    owners_keys = jax.random.split(jax.random.fold_in(key_of[7], 1), BLOCKS // BLK_DEV)
    owners_turns = jax.random.permutation(jax.random.fold_in(key_of[7], 3), BLOCKS // BLK_DEV)
    owners = jax.vmap(lambda own, number: routed_block(jax.random.fold_in(key_of[7], 2), own, number, BLK_DEV, N_ST, NPB, CAP, 2))(owners_keys, owners_turns).reshape((BLOCKS, NPB))
    slots = set_ends(ranked_ids(key_of[8], (BLOCKS, NPB), PASS_DEV, 2), jax.random.fold_in(key_of[8], 3), 0, PASS_DEV - 1).astype(jnp.int32)
    return {"queries": queries, "gate_pre": gate_pre, "cotangent": cotangent, "store": store, "store_gain": store_gain, "w_key": w_key, "w_value": w_value, "owners": owners, "slots": slots}


EPS = 1e-06

def reference(queries, gate_pre, cotangent, store, store_gain, w_key, w_value, owners, slots):
    store_rows = store.astype(jnp.float32)
    row_inverse = lax.rsqrt(lax.optimization_barrier(jnp.mean(store_rows * store_rows, axis=-1, keepdims=True)) + EPS)
    normed = (store_rows * row_inverse * store_gain).astype(jnp.bfloat16)
    key_table = jnp.dot(normed, w_key, preferred_element_type=jnp.float32).astype(jnp.bfloat16).reshape(PASSAGES, PLEN, XW)
    value_table = jnp.dot(normed, w_value, preferred_element_type=jnp.float32).astype(jnp.bfloat16).reshape(PASSAGES, PLEN, XW)
    passage_ids = (owners * PASS_DEV + slots).astype(jnp.int32)
    score_scale = HD ** (-0.5)

    def one_group(group):
        query_part, gate_part, cot_part, id_part = group
        flat_ids = id_part.reshape(-1).astype(jnp.int32)
        group_keys = key_table[flat_ids].reshape(BLK_DEV, NPB * PLEN, HEADS, HD).astype(jnp.float32)
        group_values = value_table[flat_ids].reshape(BLK_DEV, NPB * PLEN, HEADS, HD).astype(jnp.float32)
        query_wide = query_part.astype(jnp.float32)
        scores = jnp.einsum('bqhd,bkhd->bhqk', query_wide, group_keys) * score_scale
        shifted = scores - lax.optimization_barrier(jnp.max(scores, axis=-1, keepdims=True))
        weights = jnp.exp(shifted)
        weights = weights / lax.optimization_barrier(jnp.sum(weights, axis=-1, keepdims=True))
        weights_half = lax.optimization_barrier(weights.astype(jnp.bfloat16)).astype(jnp.float32)
        grad_in = jax.nn.sigmoid(gate_part.astype(jnp.float32)) * cot_part.astype(jnp.float32)
        grad_in = lax.optimization_barrier(grad_in.astype(jnp.bfloat16)).astype(jnp.float32)
        attended = jnp.einsum('bhqk,bkhd->bqhd', weights_half, group_values)
        row_delta = lax.optimization_barrier(jnp.sum(grad_in * attended, axis=-1))
        grad_weights = jnp.einsum('bqhd,bkhd->bhqk', grad_in, group_values)
        grad_scores = weights * (grad_weights - jnp.transpose(row_delta, (0, 2, 1))[..., None])
        grad_half = lax.optimization_barrier(grad_scores.astype(jnp.bfloat16)).astype(jnp.float32)
        grad_query = jnp.einsum('bhqk,bkhd->bqhd', grad_half, group_keys) * score_scale
        grad_key = jnp.einsum('bhqk,bqhd->bkhd', grad_half, query_wide) * score_scale
        grad_value = jnp.einsum('bhqk,bqhd->bkhd', weights_half, grad_in)
        return (grad_query.reshape(BLK_DEV * BLK, XW), grad_key.reshape(BLK_DEV * NPB, PLEN, XW), grad_value.reshape(BLK_DEV * NPB, PLEN, XW))
    groups = (queries.reshape(N_ST, BLK_DEV, BLK, HEADS, HD), gate_pre.reshape(N_ST, BLK_DEV, BLK, HEADS, HD), cotangent.reshape(N_ST, BLK_DEV, BLK, HEADS, HD), passage_ids.reshape(N_ST, BLK_DEV, NPB))
    grad_queries, slot_keys, slot_values = lax.map(one_group, groups)
    grad_queries = grad_queries.reshape(TOKENS, XW)
    every_id = passage_ids.reshape(-1)
    passage_keys = jnp.zeros((PASSAGES, PLEN, XW), jnp.float32).at[every_id].add(slot_keys.reshape(BLOCKS * NPB, PLEN, XW))
    passage_values = jnp.zeros((PASSAGES, PLEN, XW), jnp.float32).at[every_id].add(slot_values.reshape(BLOCKS * NPB, PLEN, XW))
    passage_keys = passage_keys.astype(jnp.bfloat16).reshape(ROWS, XW)
    passage_values = passage_values.astype(jnp.bfloat16).reshape(ROWS, XW)
    grad_normed = jnp.dot(passage_keys, w_key.T, preferred_element_type=jnp.float32) + jnp.dot(passage_values, w_value.T, preferred_element_type=jnp.float32)
    grad_w_value = jnp.dot(normed.T, passage_values, preferred_element_type=jnp.float32)
    unit_rows = store_rows * row_inverse
    grad_unit = grad_normed * store_gain
    grad_store = row_inverse * (grad_unit - unit_rows * lax.optimization_barrier(jnp.mean(grad_unit * unit_rows, axis=-1, keepdims=True)))
    return (grad_queries, grad_store, grad_w_value)
```

```python
import functools

import jax
import jax.numpy as jnp
from jax import lax
from jax.experimental import pallas as pl
from jax.experimental.pallas import tpu as pltpu
from jax.sharding import PartitionSpec as P

HD = 128
PLEN = 64


EPS = 1e-06


def row_scale(store_rows):
    return lax.rsqrt(jnp.mean(store_rows * store_rows, axis=-1, keepdims=True) + EPS)


def contract(left, right):
    return lax.dot_general(
        left, right, (((1,), (1,)), ((), ())), preferred_element_type=jnp.float32
    )


def passage_plan(queries, gate_pre, cotangent, store, store_gain, w_key, w_value, owners, slots):
    st_size = lax.axis_size("st")
    tp_size = lax.axis_size("tp")
    blocks, per_block = owners.shape
    tok_rows, local_width = queries.shape
    head_dim = HD
    local_heads = local_width // head_dim
    block_len = tok_rows // blocks
    passage_len = PLEN
    rows_dev = store.shape[0]
    passages = rows_dev // passage_len
    slot_count = blocks * per_block
    slot_cap = (2 * slot_count + st_size - 1) // st_size
    store_rows = store.astype(jnp.float32)
    row_inverse = row_scale(store_rows)
    normed = (store_rows * row_inverse * store_gain).astype(jnp.bfloat16)
    key_table = jnp.dot(normed, w_key, preferred_element_type=jnp.float32).astype(jnp.bfloat16)
    value_table = jnp.dot(normed, w_value, preferred_element_type=jnp.float32).astype(jnp.bfloat16)
    key_table = key_table.reshape(passages, passage_len, local_width)
    value_table = value_table.reshape(passages, passage_len, local_width)
    owner_flat = owners.reshape(slot_count)
    slot_flat = slots.reshape(slot_count)
    slot_order = jnp.arange(slot_count, dtype=jnp.int32)
    earlier_same = (owner_flat[:, None] == owner_flat[None, :]) & (
        slot_order[None, :] < slot_order[:, None]
    )
    slot_rank = jnp.sum(earlier_same.astype(jnp.int32), axis=1)
    position = owner_flat * slot_cap + slot_rank
    places = jnp.arange(st_size * slot_cap, dtype=jnp.int32)
    slot_hits = position[:, None] == places[None, :]
    requests = jnp.sum(jnp.where(slot_hits, slot_flat[:, None], 0), axis=0)
    requests = requests.reshape(st_size, slot_cap)
    asked_ids = lax.all_to_all(requests, "st", split_axis=0, concat_axis=0, tiled=True)
    asked_flat = asked_ids.reshape(-1)
    shape_out = asked_ids.shape + (passage_len, local_width)
    picked_keys = jnp.take(key_table, asked_flat, axis=0).reshape(shape_out)
    picked_values = jnp.take(value_table, asked_flat, axis=0).reshape(shape_out)
    sent_keys = lax.all_to_all(picked_keys, "st", split_axis=0, concat_axis=0, tiled=True)
    sent_values = lax.all_to_all(picked_values, "st", split_axis=0, concat_axis=0, tiled=True)
    got_keys, got_values, asked_ids = (sent_keys, sent_values, asked_ids)
    span = per_block * passage_len
    mine_keys = jnp.take(
        got_keys.reshape(st_size * slot_cap, passage_len, local_width), position, axis=0
    )
    mine_values = jnp.take(
        got_values.reshape(st_size * slot_cap, passage_len, local_width), position, axis=0
    )
    mine_keys = mine_keys.reshape(blocks, span, local_heads, head_dim)
    mine_values = mine_values.reshape(blocks, span, local_heads, head_dim)
    score_scale = head_dim ** (-0.5)
    query_blocks = queries.reshape(blocks, block_len, local_heads, head_dim)
    gate_open = jax.nn.sigmoid(gate_pre.astype(jnp.float32))
    grad_in = (gate_open * cotangent.astype(jnp.float32)).astype(jnp.bfloat16)
    grad_in = grad_in.reshape(blocks, block_len, local_heads, head_dim)
    scores = (
        jnp.einsum("bqhd,bkhd->bhqk", query_blocks, mine_keys, preferred_element_type=jnp.float32)
        * score_scale
    )
    shifted = scores - jnp.max(scores, axis=-1, keepdims=True)
    weights = jnp.exp(shifted)
    weights = weights / jnp.sum(weights, axis=-1, keepdims=True)
    weights_half = weights.astype(jnp.bfloat16)
    attended = jnp.einsum(
        "bhqk,bkhd->bqhd", weights_half, mine_values, preferred_element_type=jnp.float32
    )
    row_delta = jnp.sum(grad_in.astype(jnp.float32) * attended, axis=-1)
    grad_weights = jnp.einsum(
        "bqhd,bkhd->bhqk", grad_in, mine_values, preferred_element_type=jnp.float32
    )
    grad_scores = weights * (grad_weights - jnp.transpose(row_delta, (0, 2, 1))[..., None])
    grad_half = grad_scores.astype(jnp.bfloat16)
    grad_queries = (
        jnp.einsum("bhqk,bkhd->bqhd", grad_half, mine_keys, preferred_element_type=jnp.float32)
        * score_scale
    )
    grad_queries = grad_queries.reshape(tok_rows, local_width)
    grad_keys = (
        jnp.einsum("bhqk,bqhd->bkhd", grad_half, query_blocks, preferred_element_type=jnp.float32)
        * score_scale
    )
    grad_values = jnp.einsum(
        "bhqk,bqhd->bkhd", weights_half, grad_in, preferred_element_type=jnp.float32
    )
    grad_keys = grad_keys.reshape(slot_count, passage_len, local_width)
    grad_values = grad_values.reshape(slot_count, passage_len, local_width)
    empty_slots = jnp.zeros((st_size * slot_cap, passage_len, local_width), jnp.bfloat16)
    outgoing_keys = empty_slots.at[position].set(grad_keys.astype(jnp.bfloat16))
    outgoing_values = empty_slots.at[position].set(grad_values.astype(jnp.bfloat16))
    back_keys, back_values = (
        lax.all_to_all(outgoing_keys, "st", split_axis=0, concat_axis=0, tiled=True),
        lax.all_to_all(outgoing_values, "st", split_axis=0, concat_axis=0, tiled=True),
    )
    asked_flat = asked_ids.reshape(-1)
    owner_pick = (asked_flat[None, :] == jnp.arange(passages, dtype=jnp.int32)[:, None]).astype(
        jnp.bfloat16
    )
    passage_keys = jnp.dot(
        owner_pick,
        back_keys.reshape(st_size * slot_cap, passage_len * local_width),
        preferred_element_type=jnp.float32,
    )
    passage_values = jnp.dot(
        owner_pick,
        back_values.reshape(st_size * slot_cap, passage_len * local_width),
        preferred_element_type=jnp.float32,
    )
    passage_keys = passage_keys.astype(jnp.bfloat16).reshape(rows_dev, local_width)
    passage_values = passage_values.astype(jnp.bfloat16).reshape(rows_dev, local_width)
    weight_terms = lax.dot_general(
        normed, passage_values, (((0,), (0,)), ((), ())), preferred_element_type=jnp.float32
    )
    grad_w_value = lax.psum_scatter(weight_terms, "st", scatter_dimension=0, tiled=True)
    quarter = rows_dev // tp_size
    whole_key, whole_value = (
        lax.all_gather(w_key, "tp", axis=1, tiled=True),
        lax.all_gather(w_value, "tp", axis=1, tiled=True),
    )
    own_keys, own_values = (
        lax.all_to_all(passage_keys, "tp", split_axis=0, concat_axis=1, tiled=True),
        lax.all_to_all(passage_values, "tp", split_axis=0, concat_axis=1, tiled=True),
    )
    grad_normed = contract(own_keys, whole_key) + contract(own_values, whole_value)
    first_row = lax.axis_index("tp") * quarter
    own_rows = lax.dynamic_slice_in_dim(store_rows, first_row, quarter, 0)
    own_inverse = lax.dynamic_slice_in_dim(row_inverse, first_row, quarter, 0)
    unit_rows = own_rows * own_inverse
    grad_unit = grad_normed * store_gain
    grad_store = own_inverse * (
        grad_unit - unit_rows * jnp.mean(grad_unit * unit_rows, axis=-1, keepdims=True)
    )
    return (grad_queries, grad_store, grad_w_value)

FAR = 1e30
MESH = pl.DeviceIdType.MESH
NT = (((1,), (1,)), ((), ()))
TN = (((0,), (0,)), ((), ()))
CHUNK = 128


def place_of(index, n):
    odd = index % 2
    return (1 - odd) * (index // 2) + odd * (n - 1 - index // 2)


def index_at(place, n):
    place = (place + 2 * n) % n
    back = place // (n // 2)
    return (1 - back) * (2 * place) + back * (2 * (n - 1 - place) + 1)


def dot(left, right, dims=(((1,), (0,)), ((), ()))):
    return lax.dot_general(left, right, dims, preferred_element_type=jnp.float32)


def as_float(flag):
    return jnp.where(flag, jnp.float32(1.0), jnp.float32(0.0))


def rows_of_table(named, first, passages):
    total = named.shape[0]
    held = (named - first).astype(jnp.float32)
    inside = (held >= 0.0) & (held < passages)
    col = jnp.max(jnp.where(inside, held, -1.0), axis=1, keepdims=True)
    spot_col = lax.broadcasted_iota(jnp.int32, (128, 128), 0).astype(jnp.float32)
    spot_row = lax.broadcasted_iota(jnp.int32, (128, 128), 1).astype(jnp.float32)
    wide = jnp.broadcast_to(col, (total, 128))
    if total < 128:
        wide = jnp.concatenate([wide, jnp.full((128 - total, 128), 1000.0, jnp.float32)], axis=0)
    ids_row = wide.T
    key_col = wide * 128.0 + spot_col
    key_row = key_col.T
    rank_col = jnp.sum(as_float(key_row < key_col), axis=1, keepdims=True)
    rank_row = jnp.sum(as_float(key_col < key_row), axis=0, keepdims=True)
    order_row = jnp.sum(as_float(rank_col == spot_row) * spot_col, axis=0, keepdims=True)
    last_row = jnp.sum(as_float(wide <= spot_row), axis=0, keepdims=True) - 1.0
    has_row = jnp.max(as_float(wide == spot_row), axis=0, keepdims=True)
    rows = [ids_row[:1], rank_row, order_row, jnp.maximum(last_row, 0.0), has_row, jnp.zeros((3, 128), jnp.float32)]
    return jnp.concatenate(rows, axis=0).astype(jnp.int32)


IDS, RANK, ORDER, LAST, HAS = range(5)


def whole_kernel(n, tp, q_hbm, gate_hbm, cot_hbm, x_hbm, wk_hbm, wv_hbm, gain_ref, named_ref,
                 dq_ref, gs_ref, gw_ref,
                 q_all, g_all, i_all, gate_buf, cot_buf, x_buf, own_x, normed, whole, kt, vt,
                 tab_buf, tab, stats, got, joined, dq_sorted, tk, tv, pk, pv, pv_flip, own_kv,
                 dq_send, dq_recv, w_send, w_recv,
                 in_sem, x_sem, g_send, g_recv, i_send, i_recv, j_send, j_recv,
                 s_send, s_recv, ws_send, ws_recv, p_send, p_recv, t_send, t_recv, tab_sem):
    me, mine = lax.axis_index("st"), lax.axis_index("tp")
    place = place_of(me, n)
    right, left = index_at(place + 1, n), index_at(place - 1, n)
    hops = n // 2
    heads = len(q_all)
    total, block_len = q_all[0].shape[:2]
    blocks = total // n
    passages = kt[0].shape[0]
    rows_dev, features = normed.shape
    quarter = rows_dev // tp
    width = heads * HD
    feats = features // n
    scale = HD ** (-0.5)
    sibling = mine + 1 - 2 * (mine % 2)
    across = (mine + tp // 2) % tp
    half = blocks // 2

    barrier = pltpu.get_barrier_semaphore()
    for away in range(1, n):
        pl.semaphore_signal(barrier, inc=1, device_id={"st": (me + away) % n}, device_id_type=MESH)
    for away in range(1, tp):
        pl.semaphore_signal(barrier, inc=1, device_id={"tp": (mine + away) % tp}, device_id_type=MESH)

    def columns(owner, value):
        return pl.ds(pl.multiple_of(value * tp * width + owner * width, 128), width)

    loads = []
    for head in range(heads):
        loads.append(pltpu.make_async_copy(q_hbm.at[:, :, pl.ds(head * HD, HD)], q_all[head].at[pl.ds(me * blocks, blocks)], in_sem.at[head]))
    load_gate = pltpu.make_async_copy(gate_hbm, gate_buf, in_sem.at[heads])
    load_cot = pltpu.make_async_copy(cot_hbm, cot_buf, in_sem.at[heads + 1])
    load_w = [pltpu.make_async_copy(ref, whole.at[:, columns(mine, number)], in_sem.at[heads + 2 + number]) for number, ref in enumerate((wk_hbm, wv_hbm))]
    load_own = pltpu.make_async_copy(x_hbm.at[pl.ds(pl.multiple_of(mine * quarter, 16), quarter)], own_x, in_sem.at[heads + 4])

    def load_x(chunk):
        return pltpu.make_async_copy(x_hbm.at[pl.ds(chunk * CHUNK, CHUNK)], x_buf.at[chunk % 2], x_sem.at[chunk % 2])

    for copy in loads:
        copy.start()
    load_gate.start()
    load_cot.start()
    for copy in load_w:
        copy.start()
    load_x(0).start()
    load_own.start()

    sends = []

    def begin(copy):
        copy.start()
        sends.append(copy)

    def remote(src, dst, send_sem, recv_sem, **to):
        return pltpu.make_async_remote_copy(src_ref=src, dst_ref=dst, send_sem=send_sem, recv_sem=recv_sem, device_id=to, device_id_type=MESH)

    parts = ((0, 0), (0, 1), (1, 0), (1, 1))

    def gather_piece(head, side, step, part):
        number, which = parts[part]
        ref = (q_all, g_all)[number][head]
        origin = index_at(place - step, n) if side == 0 else index_at(place + step, n)
        at = ref.at[pl.ds(origin * blocks + which * half, half)]
        return remote(at, at, g_send.at[head, side, step, part], g_recv.at[head, side, step, part], st=right if side == 0 else left)

    def goes(side, step, part):
        return step < hops - 1 or parts[part][1] == side

    def ids_piece(away):
        return remote(named_ref, i_all.at[me], i_send.at[away], i_recv.at[away], st=(me + away) % n)

    def weight_piece(number, way):
        owner = mine if way < 2 else across
        at = whole.at[:, columns(owner, number)]
        return remote(at, at, t_send.at[number, way], t_recv.at[number, way], tp=across if way == 1 else sibling)

    def make_grad_in():
        load_gate.wait()
        load_cot.wait()

        @pl.loop(0, blocks)
        def _(block):
            for head in range(heads):
                cols = pl.ds(head * HD, HD)
                opened = jax.nn.sigmoid(gate_buf[block, :, cols].astype(jnp.float32))
                g_all[head][me * blocks + block] = (opened * cot_buf[block, :, cols].astype(jnp.float32)).astype(jnp.bfloat16)

    def project(chunk):
        if (chunk + 1) * CHUNK < rows_dev:
            load_x(chunk + 1).start()
        load_x(chunk).wait()
        rows = pl.ds(chunk * CHUNK, CHUNK)
        wide = x_buf[chunk % 2].astype(jnp.float32)
        ready = (wide * row_scale(wide) * gain_ref[...]).astype(jnp.bfloat16)
        normed[rows] = ready
        per = CHUNK // PLEN
        for number, table in enumerate((kt, vt)):
            out = dot(ready, whole[:, columns(mine, number)]).astype(jnp.bfloat16)
            for head in range(heads):
                table[head][pl.ds(chunk * per, per)] = out[:, head * HD:(head + 1) * HD].reshape(per, PLEN, HD)

    def make_table():
        for away in range(1, n):
            ids_piece(away).wait_recv()
        tab_buf[...] = rows_of_table(i_all[...].reshape(total, 128), me * passages, passages)
        copy = pltpu.make_async_copy(tab_buf, tab, tab_sem.at[0])
        copy.start()
        copy.wait()

    def make_stats(head, origin):
        for first in range(0, blocks, 4):
            count = min(4, blocks - first)
            spots = [origin * blocks + first + lane for lane in range(count)]
            ids = [jnp.minimum(tab[IDS, spot], passages - 1) for spot in spots]
            scores = [dot(kt[head][jnp.maximum(one, 0)], q_all[head][spot], NT) * scale for one, spot in zip(ids, spots)]
            grads = [dot(vt[head][jnp.maximum(one, 0)], g_all[head][spot], NT) for one, spot in zip(ids, spots)]
            tops = [jnp.max(one, axis=0, keepdims=True) for one in scores]
            raised = [jnp.exp(one - top) for one, top in zip(scores, tops)]
            totals = [jnp.sum(one, axis=0, keepdims=True) for one in raised]
            means = [jnp.sum(one * two, axis=0, keepdims=True) / three for one, two, three in zip(raised, grads, totals)]
            for lane in range(count):
                dead = jnp.minimum(ids[lane], 0).astype(jnp.float32) * FAR
                stats[head][origin, 0, pl.ds(first + lane, 1)] = tops[lane] + jnp.log(totals[lane]) + dead
                stats[head][origin, 1, pl.ds(first + lane, 1)] = means[lane]

    def join_piece(head, phase, away):
        peer = (me + away) % n
        at = joined[head].at[pl.ds(me * blocks, blocks)]
        return remote(
            stats[head].at[peer] if phase == 0 else at,
            got[head].at[me] if phase == 0 else at,
            j_send.at[head, phase, away], j_recv.at[head, phase, away], st=peer)

    def join_first(head):
        for away in range(1, n):
            begin(join_piece(head, 0, away))
        got[head][me] = stats[head][me]

    def join_second(head):
        for away in range(1, n):
            join_piece(head, 0, away).wait_recv()
        logs = [got[head][owner, 0] for owner in range(n)]
        top = functools.reduce(jnp.maximum, logs)
        shares = [jnp.exp(one - top) for one in logs]
        whole_sum = sum(shares)
        final = top + jnp.log(whole_sum)
        mean = sum(share * got[head][owner, 1] for owner, share in enumerate(shares)) / whole_sum
        for block in range(blocks):
            joined[head][me * blocks + block, 0:1] = final[block:block + 1]
            joined[head][me * blocks + block, 1:2] = mean[block:block + 1]
        for away in range(1, n):
            begin(join_piece(head, 1, away))

    def join_last(head):
        for away in range(1, n):
            join_piece(head, 1, away).wait_recv()

    lanes = 4

    def make_grads(head, begin_turn, end_turn, carry):
        def turn_body(turn, carry):
            acc_k, acc_v, past = carry
            spots = [jnp.clip(tab[ORDER, turn * lanes + lane], 0, total - 1) for lane in range(lanes)]
            ids = [jnp.minimum(tab[IDS, spot], passages - 1) for spot in spots]
            keys = [kt[head][jnp.maximum(one, 0)] for one in ids]
            queries = [q_all[head][spot] for spot in spots]
            givens = [g_all[head][spot] for spot in spots]
            scores = [dot(key, query, NT) * scale for key, query in zip(keys, queries)]
            grads = [dot(vt[head][jnp.maximum(one, 0)], given, NT) for one, given in zip(ids, givens)]
            weights, halves = [], []
            for one, spot, score, grad in zip(ids, spots, scores, grads):
                logs = joined[head][spot, 0:1] - jnp.minimum(one, 0).astype(jnp.float32) * FAR
                weight = jnp.exp(score - logs)
                halves.append((weight * (grad - joined[head][spot, 1:2])).astype(jnp.bfloat16))
                weights.append(weight.astype(jnp.bfloat16))
            term_k = [dot(one, query) for one, query in zip(halves, queries)]
            term_v = [dot(one, given) for one, given in zip(weights, givens)]
            steps = [dot(one, key, TN) for one, key in zip(halves, keys)]
            for lane in range(lanes):
                keep = as_float(ids[lane] == past)
                past = ids[lane]
                acc_k = acc_k * keep + term_k[lane]
                acc_v = acc_v * keep + term_v[lane]
                at = turn * lanes + lane
                tk[head][at] = (acc_k * scale).astype(jnp.bfloat16)
                tv[head][at] = acc_v.astype(jnp.bfloat16)
                dq_sorted[head][at] = (steps[lane] * scale).astype(jnp.bfloat16)
            return acc_k, acc_v, past

        return lax.fori_loop(begin_turn, end_turn, turn_body, carry)

    blank = (jnp.zeros((PLEN, HD), jnp.float32), jnp.zeros((PLEN, HD), jnp.float32), jnp.int32(-2))
    turns = total // lanes

    def pick(head):
        @pl.loop(0, passages)
        def _(passage):
            last = jnp.clip(tab[LAST, passage], 0, total - 1)
            has = tab[HAS, passage].astype(jnp.float32)
            rows = pl.ds(pl.multiple_of(passage * PLEN, PLEN), PLEN)
            pk[head][rows] = (tk[head][last].astype(jnp.float32) * has).astype(jnp.bfloat16)
            pv[head][rows] = (tv[head][last].astype(jnp.float32) * has).astype(jnp.bfloat16)

    def own_columns(owner, head, number):
        return pl.ds(pl.multiple_of(number * tp * width + owner * width + head * HD, 128), HD)

    def passage_piece(head, number, away):
        peer = (mine + away) % tp
        rows = pl.ds(pl.multiple_of(peer * quarter, 16), quarter)
        return remote((pk, pv)[number][head].at[rows], own_kv.at[:, own_columns(mine, head, number)],
                      p_send.at[head, number, away], p_recv.at[head, number, away], tp=peer)

    def share(head):
        for number in range(2):
            for away in range(1, tp):
                begin(passage_piece(head, number, away))
            rows = pl.ds(pl.multiple_of(mine * quarter, 16), quarter)
            own_kv[:, own_columns(mine, head, number)] = (pk, pv)[number][head][rows]

    dq_parts = ((0, 0), (half, 1), (half // 2, 0), (half + half // 2, 1))
    dq_count = half // 2

    def used(side, step, part):
        return step > 0 or dq_parts[part][1] == side

    def dq_piece(head, side, step, part):
        at = pl.ds(dq_parts[part][0], dq_count)
        return remote(dq_send[head].at[side, step, at], dq_recv[head].at[side, step, at],
                      s_send.at[head, side, step, part], s_recv.at[head, side, step, part], st=right if side == 0 else left)

    def dest_of(side, step):
        distance = hops - step
        return index_at(place + distance, n) if side == 0 else index_at(place - distance, n)

    def dq_step(head, step, part):
        for side in range(2):
            if not used(side, step, part):
                continue
            dest = dest_of(side, step)
            arrived = step > 0 and used(side, step - 1, part)
            if arrived:
                dq_piece(head, side, step - 1, part).wait_recv()
            for lane in range(dq_count):
                block = dq_parts[part][0] + lane
                value = dq_sorted[head][jnp.clip(tab[RANK, dest * blocks + block], 0, total - 1)]
                if arrived:
                    value = (value.astype(jnp.float32) + dq_recv[head][side, step - 1, block].astype(jnp.float32)).astype(jnp.bfloat16)
                dq_send[head][side, step, block] = value
            begin(dq_piece(head, side, step, part))

    def dq_end(head, part):
        for side in range(2):
            dq_piece(head, side, hops - 1, part).wait_recv()
        for lane in range(dq_count):
            block = dq_parts[part][0] + lane
            value = dq_sorted[head][jnp.clip(tab[RANK, me * blocks + block], 0, total - 1)].astype(jnp.float32)
            for side in range(2):
                value = value + dq_recv[head][side, hops - 1, block].astype(jnp.float32)
            dq_ref[pl.ds(block * block_len, block_len), pl.ds(head * HD, HD)] = value

    def w_piece(side, step, part):
        at = pl.ds(part * HD, HD)
        return remote(w_send.at[side, step, at], w_recv.at[side, step, at],
                      ws_send.at[side, step, part], ws_recv.at[side, step, part], st=right if side == 0 else left)

    def w_term(dest, part):
        return dot(pv_flip[pl.ds(part * HD, HD)], normed[:, pl.ds(pl.multiple_of(dest * feats, 128), feats)])

    def w_used(side, step, part):
        return step > 0 or part % 2 == side

    def w_step(step, part):
        for side in range(2):
            if not w_used(side, step, part):
                continue
            value = w_term(dest_of(side, step), part)
            at = pl.ds(part * HD, HD)
            if step > 0 and w_used(side, step - 1, part):
                w_piece(side, step - 1, part).wait_recv()
                value = value + w_recv[side, step - 1, at].astype(jnp.float32)
            w_send[side, step, at] = value.astype(jnp.bfloat16)
            begin(w_piece(side, step, part))

    def w_end(part):
        at = pl.ds(part * HD, HD)
        value = w_term(me, part)
        for side in range(2):
            w_piece(side, hops - 1, part).wait_recv()
            value = value + w_recv[side, hops - 1, at].astype(jnp.float32)
        gw_ref[:, pl.ds(part * HD, HD)] = value.T

    def flip():
        for head in range(heads):
            for first in range(0, rows_dev, 256):
                pv_flip[pl.ds(head * HD, HD), pl.ds(first, 256)] = pv[head][pl.ds(first, 256)].astype(jnp.float32).T.astype(jnp.bfloat16)

    slab = 256

    def store_slab(number):
        cols = pl.ds(number * slab, slab)
        gs_ref[:, cols] = dot(own_kv[...], whole[cols], NT) * gain_ref[:, cols]

    def store_end(first, count):
        rows = pl.ds(first, count)
        wide = own_x[rows].astype(jnp.float32)
        inverse = row_scale(wide)
        unit = wide * inverse
        value = gs_ref[rows]
        gs_ref[rows] = inverse * (value - unit * jnp.mean(value * unit, axis=-1, keepdims=True))

    for copy in loads:
        copy.wait()
    pl.semaphore_wait(barrier, n - 1 + tp - 1)
    for away in range(1, n):
        begin(ids_piece(away))
    for part in range(2):
        for side in range(2):
            begin(gather_piece(0, side, 0, part))
    for copy in load_w:
        copy.wait()
    for number in range(2):
        begin(weight_piece(number, 1))
        begin(weight_piece(number, 0))
    i_all[me] = named_ref[...]
    make_grad_in()
    for part in range(2, 4):
        for side in range(2):
            begin(gather_piece(0, side, 0, part))

    tasks = [functools.partial(project, chunk) for chunk in range(rows_dev // CHUNK)]
    tasks.append(make_table)
    tasks.append(functools.partial(make_stats, 0, me))

    def fill(count=1):
        for _ in range(count):
            if tasks:
                tasks.pop(0)()

    def arrived_at(head, step):
        return [functools.partial(make_stats, head, index_at(place - step, n)), functools.partial(make_stats, head, index_at(place + step, n))]

    state = {0: blank, 1: blank}

    def grads_task(head, first, last):
        def run():
            state[head] = make_grads(head, first, last, state[head])
        return run

    def grad_tasks(head, pieces):
        edges = [turns * piece // pieces for piece in range(pieces + 1)]
        return [grads_task(head, edges[piece], edges[piece + 1]) for piece in range(pieces)]

    def gather_step(head, step):
        for part in range(4):
            for side in range(2):
                if goes(side, step, part):
                    if step > 0:
                        gather_piece(head, side, step - 1, part).wait_recv()
                    begin(gather_piece(head, side, step, part))
            fill()

    def gather_rest(head, first):
        if first:
            for part in range(4):
                for side in range(2):
                    if not goes(side, hops - 1, part):
                        gather_piece(head, side, hops - 2, part).wait_recv()
        else:
            for part in range(4):
                gather_piece(head, parts[part][1], hops - 1, part).wait_recv()

    for step in range(1, hops):
        gather_step(0, step)
        if step > 1:
            tasks.extend(arrived_at(0, step - 1))
    for part in range(4):
        for side in range(2):
            begin(gather_piece(1, side, 0, part))
        fill()
    gather_rest(0, True)
    tasks.extend(arrived_at(0, hops - 1))
    fill(len(tasks))
    gather_rest(0, False)
    make_stats(0, index_at(place + hops, n))
    join_first(0)
    tasks.append(functools.partial(make_stats, 1, me))
    gather_step(1, 1)
    join_second(0)
    for number in range(2):
        weight_piece(number, 1).wait_recv()
        begin(weight_piece(number, 2))
    if hops > 2:
        gather_step(1, 2)
        tasks.extend(arrived_at(1, 1))
    join_last(0)
    tasks[0:0] = grad_tasks(0, 4)
    for step in range(max(3, hops - 1), hops):
        gather_step(1, step)
        tasks.extend(arrived_at(1, step - 1))
    tasks.append(functools.partial(pick, 0))
    fill(len(tasks))
    share(0)
    for part in range(4):
        dq_step(0, 0, part)
    gather_rest(1, True)
    for task in arrived_at(1, hops - 1):
        task()
    gather_rest(1, False)
    make_stats(1, index_at(place + hops, n))
    join_first(1)
    for part in range(4):
        dq_step(0, 1, part)
    join_second(1)
    for part in range(4):
        dq_step(0, 2 % hops, part) if hops > 2 else None
    join_last(1)
    tasks.extend(grad_tasks(1, 4))
    for step in range(3, hops):
        for part in range(4):
            dq_step(0, step, part)
            fill()
    fill(len(tasks))
    for part in range(4):
        dq_step(1, 0, part)
    pick(1)
    share(1)
    flip()
    for part in range(heads):
        w_step(0, part)
    for part in range(4):
        dq_end(0, part)
    for number in range(2):
        for way in (0, 2):
            weight_piece(number, way).wait_recv()
    for head in range(heads):
        for number in range(2):
            for away in range(1, tp):
                passage_piece(head, number, away).wait_recv()
    tasks.extend([functools.partial(store_slab, number) for number in range(features // slab)])
    load_own.wait()
    ending = 64
    tasks.extend([functools.partial(store_end, first, min(ending, quarter - first)) for first in range(0, quarter, ending)])
    for step in range(1, hops):
        for part in range(4):
            dq_step(1, step, part)
            fill()
        for part in range(heads):
            w_step(step, part)
    fill(len(tasks))
    for part in range(4):
        dq_end(1, part)
    for part in range(heads):
        w_end(part)
    for copy in sends:
        copy.wait_send()


def query_plan(queries, gate_pre, cotangent, store, store_gain, w_key, w_value, owners, slots):
    n = lax.axis_size("st")
    tp = lax.axis_size("tp")
    blocks, per_block = owners.shape
    tok_rows, width = queries.shape
    heads = width // HD
    block_len = tok_rows // blocks
    rows_dev, features = store.shape
    passages = rows_dev // PLEN
    quarter = rows_dev // tp
    total = n * blocks
    hops = n // 2
    feats = features // n
    named = jnp.pad(owners * passages + slots, ((0, 0), (0, 128 - per_block)), constant_values=-1)
    blocked = [one.reshape(blocks, block_len, width) for one in (queries, gate_pre, cotangent)]
    vmem = pl.BlockSpec(memory_space=pltpu.VMEM)
    anywhere = pl.BlockSpec(memory_space=pl.ANY)
    half, wide = jnp.bfloat16, jnp.float32
    dma = pltpu.SemaphoreType.DMA

    def per_head(shape, kind):
        return [pltpu.VMEM(shape, kind) for _ in range(heads)]

    return pl.pallas_call(
        functools.partial(whole_kernel, n, tp),
        out_shape=(
            jax.ShapeDtypeStruct((tok_rows, width), wide),
            jax.ShapeDtypeStruct((quarter, features), wide),
            jax.ShapeDtypeStruct((feats, width), wide),
        ),
        in_specs=[anywhere] * 6 + [vmem] * 2,
        out_specs=(vmem,) * 3,
        scratch_shapes=[
            per_head((total, block_len, HD), half),
            per_head((total, block_len, HD), half),
            pltpu.VMEM((n, blocks, 128), jnp.int32),
            pltpu.VMEM((blocks, block_len, width), half),
            pltpu.VMEM((blocks, block_len, width), half),
            pltpu.VMEM((2, CHUNK, features), half),
            pltpu.VMEM((quarter, features), half),
            pltpu.VMEM((rows_dev, features), half),
            pltpu.VMEM((features, 2 * tp * width), half),
            per_head((passages, PLEN, HD), half),
            per_head((passages, PLEN, HD), half),
            pltpu.VMEM((8, 128), jnp.int32),
            pltpu.SMEM((8, 128), jnp.int32),
            per_head((n + 1, 2, blocks, block_len), wide),
            per_head((n, 2, blocks, block_len), wide),
            per_head((total + 4, 2, block_len), wide),
            per_head((total, block_len, HD), half),
            per_head((total, PLEN, HD), half),
            per_head((total, PLEN, HD), half),
            per_head((rows_dev, HD), half),
            per_head((rows_dev, HD), half),
            pltpu.VMEM((width, rows_dev), half),
            pltpu.VMEM((quarter, 2 * tp * width), half),
            per_head((2, hops, blocks, block_len, HD), half),
            per_head((2, hops, blocks, block_len, HD), half),
            pltpu.VMEM((2, hops, width, feats), half),
            pltpu.VMEM((2, hops, width, feats), half),
            dma((heads + 5,)),
            dma((2,)),
            dma((heads, 2, hops, 4)),
            dma((heads, 2, hops, 4)),
            dma((n,)),
            dma((n,)),
            dma((heads, 2, n)),
            dma((heads, 2, n)),
            dma((heads, 2, hops, 4)),
            dma((heads, 2, hops, 4)),
            dma((2, hops, heads)),
            dma((2, hops, heads)),
            dma((heads, 2, tp)),
            dma((heads, 2, tp)),
            dma((2, 3)),
            dma((2, 3)),
            dma((1,)),
        ],
        cost_estimate=pl.CostEstimate(flops=2 * 10**10, bytes_accessed=3 * 10**7, transcendentals=0),
        compiler_params=pltpu.CompilerParams(collective_id=0, has_side_effects=True, vmem_limit_bytes=60 << 20),
        name="whole",
    )(*blocked, store, w_key, w_value, store_gain[None], named)


def fits(queries, store, owners):
    n, tp = lax.axis_size("st"), lax.axis_size("tp")
    blocks = owners.shape[0]
    block_len = queries.shape[0] // blocks
    slot_cap = (2 * owners.size + n - 1) // n
    return (
        n % 2 == 0 and n >= 8 and tp == 4 and blocks == 8 and n * blocks <= 128
        and block_len == 128 and queries.shape[1] == 2 * HD
        and store.shape[0] % (tp * CHUNK // 2) == 0 and store.shape[0] % 256 == 0
        and store.shape[0] // PLEN <= 128 and store.shape[1] % (256 * n) == 0
        and 8 * slot_cap * PLEN >= 3 * queries.shape[0]
    )


def local(*arrays):
    if fits(arrays[0], arrays[3], arrays[7]):
        return query_plan(*arrays)
    return passage_plan(*arrays)


def solution(mesh):
    placed = (
        P("st", "tp"),
        P("st", "tp"),
        P("st", "tp"),
        P("st", None),
        P(),
        P(None, "tp"),
        P(None, "tp"),
        P("st", None),
        P("st", None),
    )
    return jax.shard_map(
        local,
        mesh=mesh,
        in_specs=placed,
        out_specs=(P("st", "tp"), P(("st", "tp"), None), P("st", "tp")),
        check_vma=False,
    )
```

```python
import functools

import jax
import jax.numpy as jnp
from jax import lax
from jax.experimental import pallas as pl
from jax.experimental.pallas import tpu as pltpu
from jax.sharding import PartitionSpec as P

HD = 128
PLEN = 64


EPS = 1e-06


def row_scale(store_rows):
    return lax.rsqrt(jnp.mean(store_rows * store_rows, axis=-1, keepdims=True) + EPS)


def contract(left, right):
    return lax.dot_general(
        left, right, (((1,), (1,)), ((), ())), preferred_element_type=jnp.float32
    )


def passage_plan(queries, gate_pre, cotangent, store, store_gain, w_key, w_value, owners, slots):
    st_size = lax.axis_size("st")
    tp_size = lax.axis_size("tp")
    blocks, per_block = owners.shape
    tok_rows, local_width = queries.shape
    head_dim = HD
    local_heads = local_width // head_dim
    block_len = tok_rows // blocks
    passage_len = PLEN
    rows_dev = store.shape[0]
    passages = rows_dev // passage_len
    slot_count = blocks * per_block
    slot_cap = (2 * slot_count + st_size - 1) // st_size
    store_rows = store.astype(jnp.float32)
    row_inverse = row_scale(store_rows)
    normed = (store_rows * row_inverse * store_gain).astype(jnp.bfloat16)
    key_table = jnp.dot(normed, w_key, preferred_element_type=jnp.float32).astype(jnp.bfloat16)
    value_table = jnp.dot(normed, w_value, preferred_element_type=jnp.float32).astype(jnp.bfloat16)
    key_table = key_table.reshape(passages, passage_len, local_width)
    value_table = value_table.reshape(passages, passage_len, local_width)
    owner_flat = owners.reshape(slot_count)
    slot_flat = slots.reshape(slot_count)
    slot_order = jnp.arange(slot_count, dtype=jnp.int32)
    earlier_same = (owner_flat[:, None] == owner_flat[None, :]) & (
        slot_order[None, :] < slot_order[:, None]
    )
    slot_rank = jnp.sum(earlier_same.astype(jnp.int32), axis=1)
    position = owner_flat * slot_cap + slot_rank
    places = jnp.arange(st_size * slot_cap, dtype=jnp.int32)
    slot_hits = position[:, None] == places[None, :]
    requests = jnp.sum(jnp.where(slot_hits, slot_flat[:, None], 0), axis=0)
    requests = requests.reshape(st_size, slot_cap)
    asked_ids = lax.all_to_all(requests, "st", split_axis=0, concat_axis=0, tiled=True)
    asked_flat = asked_ids.reshape(-1)
    shape_out = asked_ids.shape + (passage_len, local_width)
    picked_keys = jnp.take(key_table, asked_flat, axis=0).reshape(shape_out)
    picked_values = jnp.take(value_table, asked_flat, axis=0).reshape(shape_out)
    sent_keys = lax.all_to_all(picked_keys, "st", split_axis=0, concat_axis=0, tiled=True)
    sent_values = lax.all_to_all(picked_values, "st", split_axis=0, concat_axis=0, tiled=True)
    got_keys, got_values, asked_ids = (sent_keys, sent_values, asked_ids)
    span = per_block * passage_len
    mine_keys = jnp.take(
        got_keys.reshape(st_size * slot_cap, passage_len, local_width), position, axis=0
    )
    mine_values = jnp.take(
        got_values.reshape(st_size * slot_cap, passage_len, local_width), position, axis=0
    )
    mine_keys = mine_keys.reshape(blocks, span, local_heads, head_dim)
    mine_values = mine_values.reshape(blocks, span, local_heads, head_dim)
    score_scale = head_dim ** (-0.5)
    query_blocks = queries.reshape(blocks, block_len, local_heads, head_dim)
    gate_open = jax.nn.sigmoid(gate_pre.astype(jnp.float32))
    grad_in = (gate_open * cotangent.astype(jnp.float32)).astype(jnp.bfloat16)
    grad_in = grad_in.reshape(blocks, block_len, local_heads, head_dim)
    scores = (
        jnp.einsum("bqhd,bkhd->bhqk", query_blocks, mine_keys, preferred_element_type=jnp.float32)
        * score_scale
    )
    shifted = scores - jnp.max(scores, axis=-1, keepdims=True)
    weights = jnp.exp(shifted)
    weights = weights / jnp.sum(weights, axis=-1, keepdims=True)
    weights_half = weights.astype(jnp.bfloat16)
    attended = jnp.einsum(
        "bhqk,bkhd->bqhd", weights_half, mine_values, preferred_element_type=jnp.float32
    )
    row_delta = jnp.sum(grad_in.astype(jnp.float32) * attended, axis=-1)
    grad_weights = jnp.einsum(
        "bqhd,bkhd->bhqk", grad_in, mine_values, preferred_element_type=jnp.float32
    )
    grad_scores = weights * (grad_weights - jnp.transpose(row_delta, (0, 2, 1))[..., None])
    grad_half = grad_scores.astype(jnp.bfloat16)
    grad_queries = (
        jnp.einsum("bhqk,bkhd->bqhd", grad_half, mine_keys, preferred_element_type=jnp.float32)
        * score_scale
    )
    grad_queries = grad_queries.reshape(tok_rows, local_width)
    grad_keys = (
        jnp.einsum("bhqk,bqhd->bkhd", grad_half, query_blocks, preferred_element_type=jnp.float32)
        * score_scale
    )
    grad_values = jnp.einsum(
        "bhqk,bqhd->bkhd", weights_half, grad_in, preferred_element_type=jnp.float32
    )
    grad_keys = grad_keys.reshape(slot_count, passage_len, local_width)
    grad_values = grad_values.reshape(slot_count, passage_len, local_width)
    empty_slots = jnp.zeros((st_size * slot_cap, passage_len, local_width), jnp.bfloat16)
    outgoing_keys = empty_slots.at[position].set(grad_keys.astype(jnp.bfloat16))
    outgoing_values = empty_slots.at[position].set(grad_values.astype(jnp.bfloat16))
    back_keys, back_values = (
        lax.all_to_all(outgoing_keys, "st", split_axis=0, concat_axis=0, tiled=True),
        lax.all_to_all(outgoing_values, "st", split_axis=0, concat_axis=0, tiled=True),
    )
    asked_flat = asked_ids.reshape(-1)
    owner_pick = (asked_flat[None, :] == jnp.arange(passages, dtype=jnp.int32)[:, None]).astype(
        jnp.bfloat16
    )
    passage_keys = jnp.dot(
        owner_pick,
        back_keys.reshape(st_size * slot_cap, passage_len * local_width),
        preferred_element_type=jnp.float32,
    )
    passage_values = jnp.dot(
        owner_pick,
        back_values.reshape(st_size * slot_cap, passage_len * local_width),
        preferred_element_type=jnp.float32,
    )
    passage_keys = passage_keys.astype(jnp.bfloat16).reshape(rows_dev, local_width)
    passage_values = passage_values.astype(jnp.bfloat16).reshape(rows_dev, local_width)
    weight_terms = lax.dot_general(
        normed, passage_values, (((0,), (0,)), ((), ())), preferred_element_type=jnp.float32
    )
    grad_w_value = lax.psum_scatter(weight_terms, "st", scatter_dimension=0, tiled=True)
    quarter = rows_dev // tp_size
    whole_key, whole_value = (
        lax.all_gather(w_key, "tp", axis=1, tiled=True),
        lax.all_gather(w_value, "tp", axis=1, tiled=True),
    )
    own_keys, own_values = (
        lax.all_to_all(passage_keys, "tp", split_axis=0, concat_axis=1, tiled=True),
        lax.all_to_all(passage_values, "tp", split_axis=0, concat_axis=1, tiled=True),
    )
    grad_normed = contract(own_keys, whole_key) + contract(own_values, whole_value)
    first_row = lax.axis_index("tp") * quarter
    own_rows = lax.dynamic_slice_in_dim(store_rows, first_row, quarter, 0)
    own_inverse = lax.dynamic_slice_in_dim(row_inverse, first_row, quarter, 0)
    unit_rows = own_rows * own_inverse
    grad_unit = grad_normed * store_gain
    grad_store = own_inverse * (
        grad_unit - unit_rows * jnp.mean(grad_unit * unit_rows, axis=-1, keepdims=True)
    )
    return (grad_queries, grad_store, grad_w_value)

FAR = 1e30
MESH = pl.DeviceIdType.MESH
NT = (((1,), (1,)), ((), ()))
TN = (((0,), (0,)), ((), ()))
CHUNK = 128
VMEM_LIMIT = 45 << 20


def place_of(index, n):
    odd = index % 2
    return (1 - odd) * (index // 2) + odd * (n - 1 - index // 2)


def index_at(place, n):
    place = (place + 2 * n) % n
    back = place // (n // 2)
    return (1 - back) * (2 * place) + back * (2 * (n - 1 - place) + 1)


def dot(left, right, dims=(((1,), (0,)), ((), ()))):
    return lax.dot_general(left, right, dims, preferred_element_type=jnp.float32)


def as_float(flag):
    return jnp.where(flag, jnp.float32(1.0), jnp.float32(0.0))


def rows_of_table(named, first, passages):
    total = named.shape[0]
    held = (named - first).astype(jnp.float32)
    inside = (held >= 0.0) & (held < passages)
    col = jnp.max(jnp.where(inside, held, -1.0), axis=1, keepdims=True)
    spot_col = lax.broadcasted_iota(jnp.int32, (128, 128), 0).astype(jnp.float32)
    spot_row = lax.broadcasted_iota(jnp.int32, (128, 128), 1).astype(jnp.float32)
    wide = jnp.broadcast_to(col, (total, 128))
    if total < 128:
        wide = jnp.concatenate([wide, jnp.full((128 - total, 128), 1000.0, jnp.float32)], axis=0)
    ids_row = wide.T
    key_col = wide * 128.0 + spot_col
    key_row = key_col.T
    rank_col = jnp.sum(as_float(key_row < key_col), axis=1, keepdims=True)
    rank_row = jnp.sum(as_float(key_col < key_row), axis=0, keepdims=True)
    order_row = jnp.sum(as_float(rank_col == spot_row) * spot_col, axis=0, keepdims=True)
    last_row = jnp.sum(as_float(wide <= spot_row), axis=0, keepdims=True) - 1.0
    has_row = jnp.max(as_float(wide == spot_row), axis=0, keepdims=True)
    rows = [ids_row[:1], rank_row, order_row, jnp.maximum(last_row, 0.0), has_row, jnp.zeros((3, 128), jnp.float32)]
    return jnp.concatenate(rows, axis=0).astype(jnp.int32)


IDS, RANK, ORDER, LAST, HAS = range(5)


def whole_kernel(n, tp, q_hbm, gate_hbm, cot_hbm, x_hbm, wk_hbm, wv_hbm, gain_hbm, owners_hbm, slots_hbm,
                 dq_ref, gs_ref, gw_ref,
                 gain_ref, owners_buf, slots_buf, flat, named_ref, q_all, g_all, i_all, gate_buf, cot_buf, x_buf, own_x, normed, whole, kt, vt,
                 tab_buf, tab, stats, got, joined, dq_sorted, tk, tv, pk, pv, pv_flip, own_kv,
                 dq_send, dq_recv, w_send, w_recv,
                 in_sem, x_sem, g_send, g_recv, i_send, i_recv, j_send, j_recv,
                 s_send, s_recv, ws_send, ws_recv, p_send, p_recv, t_send, t_recv, tab_sem):
    me, mine = lax.axis_index("st"), lax.axis_index("tp")
    place = place_of(me, n)
    right, left = index_at(place + 1, n), index_at(place - 1, n)
    hops = n // 2
    heads = len(q_all)
    total, block_len = q_all[0].shape[:2]
    blocks = total // n
    passages = kt[0].shape[0]
    rows_dev, features = normed.shape
    quarter = rows_dev // tp
    width = heads * HD
    feats = features // n
    scale = HD ** (-0.5)
    sibling = mine + 1 - 2 * (mine % 2)
    across = (mine + tp // 2) % tp
    half = blocks // 2

    barrier = pltpu.get_barrier_semaphore()
    for away in range(1, n):
        pl.semaphore_signal(barrier, inc=1, device_id={"st": (me + away) % n}, device_id_type=MESH)
    for away in range(1, tp):
        pl.semaphore_signal(barrier, inc=1, device_id={"tp": (mine + away) % tp}, device_id_type=MESH)

    def columns(owner, value):
        return pl.ds(pl.multiple_of(value * tp * width + owner * width, 128), width)

    loads = []
    for head in range(heads):
        loads.append(pltpu.make_async_copy(q_hbm.at[:, :, pl.ds(head * HD, HD)], q_all[head].at[pl.ds(me * blocks, blocks)], in_sem.at[head]))
    load_gate = pltpu.make_async_copy(gate_hbm, gate_buf, in_sem.at[heads])
    load_cot = pltpu.make_async_copy(cot_hbm, cot_buf, in_sem.at[heads + 1])
    load_w = [pltpu.make_async_copy(ref, whole.at[:, columns(mine, number)], in_sem.at[heads + 2 + number]) for number, ref in enumerate((wk_hbm, wv_hbm))]
    load_small = [pltpu.make_async_copy(src, dst, in_sem.at[heads + 5 + number]) for number, (src, dst) in enumerate(((owners_hbm, owners_buf), (slots_hbm, slots_buf), (gain_hbm, gain_ref)))]
    load_own = pltpu.make_async_copy(x_hbm.at[pl.ds(pl.multiple_of(mine * quarter, 16), quarter)], own_x, in_sem.at[heads + 4])

    def load_x(chunk):
        return pltpu.make_async_copy(x_hbm.at[pl.ds(chunk * CHUNK, CHUNK)], x_buf.at[chunk % 2], x_sem.at[chunk % 2])

    for copy in load_small[:2] + loads + [load_gate, load_cot] + load_w + load_small[2:] + [load_x(0), load_own]:
        copy.start()

    sends = []

    def begin(copy):
        copy.start()
        sends.append(copy)

    def remote(src, dst, send_sem, recv_sem, **to):
        return pltpu.make_async_remote_copy(src_ref=src, dst_ref=dst, send_sem=send_sem, recv_sem=recv_sem, device_id=to, device_id_type=MESH)

    parts = ((0, 0), (0, 1), (1, 0), (1, 1))

    def gather_piece(head, side, step, part):
        number, which = parts[part]
        ref = (q_all, g_all)[number][head]
        origin = index_at(place - step, n) if side == 0 else index_at(place + step, n)
        at = ref.at[pl.ds(origin * blocks + which * half, half)]
        return remote(at, at, g_send.at[head, side, step, part], g_recv.at[head, side, step, part], st=right if side == 0 else left)

    def goes(side, step, part):
        return step < hops - 1 or parts[part][1] == side

    def ids_piece(away):
        return remote(named_ref, i_all.at[me], i_send.at[away], i_recv.at[away], st=(me + away) % n)

    def weight_piece(number, way):
        owner = mine if way < 2 else across
        at = whole.at[:, columns(owner, number)]
        return remote(at, at, t_send.at[number, way], t_recv.at[number, way], tp=across if way == 1 else sibling)

    def make_grad_in():
        load_gate.wait()
        load_cot.wait()

        @pl.loop(0, blocks)
        def _(block):
            for head in range(heads):
                cols = pl.ds(head * HD, HD)
                opened = jax.nn.sigmoid(gate_buf[block, :, cols].astype(jnp.float32))
                g_all[head][me * blocks + block] = (opened * cot_buf[block, :, cols].astype(jnp.float32)).astype(jnp.bfloat16)

    def project(chunk):
        if (chunk + 1) * CHUNK < rows_dev:
            load_x(chunk + 1).start()
        load_x(chunk).wait()
        rows = pl.ds(chunk * CHUNK, CHUNK)
        wide = x_buf[chunk % 2].astype(jnp.float32)
        ready = (wide * row_scale(wide) * gain_ref[...]).astype(jnp.bfloat16)
        normed[rows] = ready
        per = CHUNK // PLEN
        for number, table in enumerate((kt, vt)):
            out = dot(ready, whole[:, columns(mine, number)]).astype(jnp.bfloat16)
            for head in range(heads):
                table[head][pl.ds(chunk * per, per)] = out[:, head * HD:(head + 1) * HD].reshape(per, PLEN, HD)

    def make_table():
        for away in range(1, n):
            ids_piece(away).wait_recv()
        tab_buf[...] = rows_of_table(i_all[...].reshape(total, 128), me * passages, passages)
        copy = pltpu.make_async_copy(tab_buf, tab, tab_sem.at[0])
        copy.start()
        copy.wait()

    def make_stats(head, origin):
        for first in range(0, blocks, 4):
            count = min(4, blocks - first)
            spots = [origin * blocks + first + lane for lane in range(count)]
            ids = [jnp.minimum(tab[IDS, spot], passages - 1) for spot in spots]
            scores = [dot(kt[head][jnp.maximum(one, 0)], q_all[head][spot], NT) * scale for one, spot in zip(ids, spots)]
            grads = [dot(vt[head][jnp.maximum(one, 0)], g_all[head][spot], NT) for one, spot in zip(ids, spots)]
            tops = [jnp.max(one, axis=0, keepdims=True) for one in scores]
            raised = [jnp.exp(one - top) for one, top in zip(scores, tops)]
            totals = [jnp.sum(one, axis=0, keepdims=True) for one in raised]
            means = [jnp.sum(one * two, axis=0, keepdims=True) / three for one, two, three in zip(raised, grads, totals)]
            for lane in range(count):
                dead = jnp.minimum(ids[lane], 0).astype(jnp.float32) * FAR
                stats[head][origin, 0, pl.ds(first + lane, 1)] = tops[lane] + jnp.log(totals[lane]) + dead
                stats[head][origin, 1, pl.ds(first + lane, 1)] = means[lane]

    def join_piece(head, phase, away):
        peer = (me + away) % n
        at = joined[head].at[pl.ds(me * blocks, blocks)]
        return remote(
            stats[head].at[peer] if phase == 0 else at,
            got[head].at[me] if phase == 0 else at,
            j_send.at[head, phase, away], j_recv.at[head, phase, away], st=peer)

    def join_first(head):
        for away in range(1, n):
            begin(join_piece(head, 0, away))
        got[head][me] = stats[head][me]

    def join_second(head):
        for away in range(1, n):
            join_piece(head, 0, away).wait_recv()
        logs = [got[head][owner, 0] for owner in range(n)]
        top = functools.reduce(jnp.maximum, logs)
        shares = [jnp.exp(one - top) for one in logs]
        whole_sum = sum(shares)
        final = top + jnp.log(whole_sum)
        mean = sum(share * got[head][owner, 1] for owner, share in enumerate(shares)) / whole_sum
        for block in range(blocks):
            joined[head][me * blocks + block, 0:1] = final[block:block + 1]
            joined[head][me * blocks + block, 1:2] = mean[block:block + 1]
        for away in range(1, n):
            begin(join_piece(head, 1, away))

    def join_last(head):
        for away in range(1, n):
            join_piece(head, 1, away).wait_recv()

    lanes = 4

    def make_grads(head, begin_turn, end_turn, carry):
        def turn_body(turn, carry):
            acc_k, acc_v, past = carry
            spots = [jnp.clip(tab[ORDER, turn * lanes + lane], 0, total - 1) for lane in range(lanes)]
            ids = [jnp.minimum(tab[IDS, spot], passages - 1) for spot in spots]
            keys = [kt[head][jnp.maximum(one, 0)] for one in ids]
            queries = [q_all[head][spot] for spot in spots]
            givens = [g_all[head][spot] for spot in spots]
            scores = [dot(key, query, NT) * scale for key, query in zip(keys, queries)]
            grads = [dot(vt[head][jnp.maximum(one, 0)], given, NT) for one, given in zip(ids, givens)]
            weights, halves = [], []
            for one, spot, score, grad in zip(ids, spots, scores, grads):
                logs = joined[head][spot, 0:1] - jnp.minimum(one, 0).astype(jnp.float32) * FAR
                weight = jnp.exp(score - logs)
                halves.append((weight * (grad - joined[head][spot, 1:2])).astype(jnp.bfloat16))
                weights.append(weight.astype(jnp.bfloat16))
            term_k = [dot(one, query) for one, query in zip(halves, queries)]
            term_v = [dot(one, given) for one, given in zip(weights, givens)]
            steps = [dot(one, key, TN) for one, key in zip(halves, keys)]
            for lane in range(lanes):
                keep = as_float(ids[lane] == past)
                past = ids[lane]
                acc_k = acc_k * keep + term_k[lane]
                acc_v = acc_v * keep + term_v[lane]
                at = turn * lanes + lane
                tk[at] = (acc_k * scale).astype(jnp.bfloat16)
                tv[at] = acc_v.astype(jnp.bfloat16)
                dq_sorted[head][at] = (steps[lane] * scale).astype(jnp.bfloat16)
            return acc_k, acc_v, past

        return lax.fori_loop(begin_turn, end_turn, turn_body, carry)

    blank = (jnp.zeros((PLEN, HD), jnp.float32), jnp.zeros((PLEN, HD), jnp.float32), jnp.int32(-2))
    turns = total // lanes

    def pick(head):
        @pl.loop(0, passages)
        def _(passage):
            last = jnp.clip(tab[LAST, passage], 0, total - 1)
            has = tab[HAS, passage].astype(jnp.float32)
            rows = pl.ds(pl.multiple_of(passage * PLEN, PLEN), PLEN)
            pk[head][rows] = (tk[last].astype(jnp.float32) * has).astype(jnp.bfloat16)
            pv[head][rows] = (tv[last].astype(jnp.float32) * has).astype(jnp.bfloat16)

    def own_columns(owner, head, number):
        return pl.ds(pl.multiple_of(number * tp * width + owner * width + head * HD, 128), HD)

    def passage_piece(head, number, away):
        peer = (mine + away) % tp
        rows = pl.ds(pl.multiple_of(peer * quarter, 16), quarter)
        return remote((pk, pv)[number][head].at[rows], own_kv.at[:, own_columns(mine, head, number)],
                      p_send.at[head, number, away], p_recv.at[head, number, away], tp=peer)

    def share(head):
        for number in range(2):
            for away in range(1, tp):
                begin(passage_piece(head, number, away))
            rows = pl.ds(pl.multiple_of(mine * quarter, 16), quarter)
            own_kv[:, own_columns(mine, head, number)] = (pk, pv)[number][head][rows]

    dq_parts = ((0, 0), (half, 1), (half // 2, 0), (half + half // 2, 1))
    dq_count = half // 2

    def used(side, step, part):
        return step > 0 or dq_parts[part][1] == side

    def dq_piece(head, side, step, part):
        at = pl.ds(dq_parts[part][0], dq_count)
        src = dq_recv[head].at[side, step - 1, at] if step > 0 else dq_send[head].at[at]
        return remote(src, dq_recv[head].at[side, step, at],
                      s_send.at[head, side, step, part], s_recv.at[head, side, step, part], st=right if side == 0 else left)

    def dest_of(side, step):
        distance = hops - step
        return index_at(place + distance, n) if side == 0 else index_at(place - distance, n)

    def dq_step(head, step, part):
        for side in range(2):
            if not used(side, step, part):
                continue
            dest = dest_of(side, step)
            arrived = step > 0 and used(side, step - 1, part)
            if arrived:
                dq_piece(head, side, step - 1, part).wait_recv()
            for lane in range(dq_count):
                block = dq_parts[part][0] + lane
                value = dq_sorted[head][jnp.clip(tab[RANK, dest * blocks + block], 0, total - 1)]
                if arrived:
                    value = (value.astype(jnp.float32) + dq_recv[head][side, step - 1, block].astype(jnp.float32)).astype(jnp.bfloat16)
                if step > 0:
                    dq_recv[head][side, step - 1, block] = value
                else:
                    dq_send[head][block] = value
            begin(dq_piece(head, side, step, part))

    def dq_end(head, part):
        for side in range(2):
            dq_piece(head, side, hops - 1, part).wait_recv()
        for lane in range(dq_count):
            block = dq_parts[part][0] + lane
            value = dq_sorted[head][jnp.clip(tab[RANK, me * blocks + block], 0, total - 1)].astype(jnp.float32)
            for side in range(2):
                value = value + dq_recv[head][side, hops - 1, block].astype(jnp.float32)
            dq_ref[pl.ds(block * block_len, block_len), pl.ds(head * HD, HD)] = value

    def w_piece(side, step, part):
        src = w_recv.at[side, step - 1, part] if step > 0 else w_send.at[part]
        return remote(src, w_recv.at[side, step, part],
                      ws_send.at[side, step, part], ws_recv.at[side, step, part], st=right if side == 0 else left)

    def w_term(dest, part):
        return dot(pv_flip[part], normed[:, pl.ds(pl.multiple_of(dest * feats, 128), feats)])

    def w_used(side, step, part):
        return step > 0 or part % 2 == side

    def w_step(step, part):
        for side in range(2):
            if not w_used(side, step, part):
                continue
            value = w_term(dest_of(side, step), part)
            if step > 0 and w_used(side, step - 1, part):
                w_piece(side, step - 1, part).wait_recv()
                value = value + w_recv[side, step - 1, part].astype(jnp.float32)
            if step > 0:
                w_recv[side, step - 1, part] = value.astype(jnp.bfloat16)
            else:
                w_send[part] = value.astype(jnp.bfloat16)
            begin(w_piece(side, step, part))

    def w_end(part):
        value = w_term(me, part)
        for side in range(2):
            w_piece(side, hops - 1, part).wait_recv()
            value = value + w_recv[side, hops - 1, part].astype(jnp.float32)
        gw_ref[:, pl.ds(part * HD, HD)] = value.T

    def flip(head):
        for first in range(0, rows_dev, 256):
            pv_flip[head, :, pl.ds(first, 256)] = pv[head][pl.ds(first, 256)].astype(jnp.float32).T.astype(jnp.bfloat16)

    slab = 256

    def store_slab(number):
        cols = pl.ds(number * slab, slab)
        gs_ref[:, cols] = dot(own_kv[...], whole[cols], NT) * gain_ref[:, cols]

    def store_end(first, count):
        rows = pl.ds(first, count)
        wide = own_x[rows].astype(jnp.float32)
        inverse = row_scale(wide)
        unit = wide * inverse
        value = gs_ref[rows]
        gs_ref[rows] = inverse * (value - unit * jnp.mean(value * unit, axis=-1, keepdims=True))

    for copy in load_small[:2]:
        copy.wait()
    per_block = owners_buf.shape[0]
    flat[...] = jnp.full(flat.shape, -1.0, jnp.float32)
    flat[pl.ds(0, per_block), pl.ds(0, blocks)] = (owners_buf[...] * passages + slots_buf[...]).astype(jnp.float32)
    named_ref[...] = jnp.full(named_ref.shape, -1, jnp.int32)
    named_ref[:, pl.ds(0, 8)] = flat[...].T[:blocks].astype(jnp.int32)
    loads[0].wait()
    pl.semaphore_wait(barrier, n - 1 + tp - 1)
    for part in range(2):
        for side in range(2):
            begin(gather_piece(0, side, 0, part))
    make_grad_in()
    for part in range(2, 4):
        for side in range(2):
            begin(gather_piece(0, side, 0, part))
    for away in range(1, n):
        begin(ids_piece(away))
    i_all[me] = named_ref[...]
    for copy in load_w:
        copy.wait()
    for number in range(2):
        begin(weight_piece(number, 1))
        begin(weight_piece(number, 0))
    load_small[2].wait()
    for copy in loads[1:]:
        copy.wait()

    tasks = [functools.partial(project, chunk) for chunk in range(rows_dev // CHUNK)]
    tasks.append(make_table)
    tasks.append(functools.partial(make_stats, 0, me))

    def idle():
        pass

    def fill(count=1):
        for _ in range(count):
            if tasks:
                tasks.pop(0)()

    def both(head, step):
        def run():
            make_stats(head, index_at(place - step, n))
            make_stats(head, index_at(place + step, n))
        return run

    state = {0: blank, 1: blank}

    def grads_task(head, first, last):
        def run():
            state[head] = make_grads(head, first, last, state[head])
        return run

    def grad_tasks(head, pieces):
        edges = [turns * piece // pieces for piece in range(pieces + 1)]
        return [grads_task(head, edges[piece], edges[piece + 1]) for piece in range(pieces)]

    def gather_step(head, step):
        for part in range(4):
            for side in range(2):
                if goes(side, step, part):
                    if step > 0:
                        gather_piece(head, side, step - 1, part).wait_recv()
                    begin(gather_piece(head, side, step, part))
            fill()

    def gather_rest(head, first):
        if first:
            for part in range(4):
                for side in range(2):
                    if not goes(side, hops - 1, part):
                        gather_piece(head, side, hops - 2, part).wait_recv()
        else:
            for part in range(4):
                gather_piece(head, parts[part][1], hops - 1, part).wait_recv()

    def forward_weights():
        for number in range(2):
            weight_piece(number, 1).wait_recv()
            begin(weight_piece(number, 2))

    for step in range(1, hops):
        gather_step(0, step)
        if step < hops - 1:
            tasks.append(both(0, step))
    for part in range(4):
        for side in range(2):
            begin(gather_piece(1, side, 0, part))
        fill()
    gather_rest(0, True)
    tasks.append(both(0, hops - 1))
    fill(len(tasks))
    gather_rest(0, False)
    make_stats(0, index_at(place + hops, n))
    join_first(0)
    tasks.extend([functools.partial(make_stats, 1, me), idle, functools.partial(join_second, 0), forward_weights])
    gather_step(1, 1)
    tasks.extend([both(1, 1), idle, idle, functools.partial(join_last, 0)])
    gather_step(1, 2)
    tasks.extend(grad_tasks(0, 4))
    tasks.extend([functools.partial(pick, 0), functools.partial(share, 0), functools.partial(flip, 0)])
    for step in range(3, hops):
        gather_step(1, step)
    fill(len(tasks))
    for part in range(4):
        dq_step(0, 0, part)
    for step in range(2, hops - 1):
        both(1, step)()
    gather_rest(1, True)
    both(1, hops - 1)()
    gather_rest(1, False)
    make_stats(1, index_at(place + hops, n))
    join_first(1)
    w_step(0, 0)
    for part in range(4):
        dq_step(0, 1, part)
    join_second(1)
    w_step(1, 0)
    for part in range(4):
        dq_step(0, 2, part)
    join_last(1)
    tasks.extend(grad_tasks(1, 8))
    for step in range(3, hops):
        for part in range(4):
            dq_step(0, step, part)
            fill(2)
    fill(len(tasks))
    for part in range(4):
        dq_step(1, 0, part)
    w_step(2, 0)
    pick(1)
    share(1)
    flip(1)
    w_step(0, 1)
    for part in range(4):
        dq_end(0, part)
    w_step(3, 0)
    for part in range(4):
        dq_step(1, 1, part)
    w_step(1, 1)
    for number in range(2):
        for way in (0, 2):
            weight_piece(number, way).wait_recv()
    for head in range(heads):
        for number in range(2):
            for away in range(1, tp):
                passage_piece(head, number, away).wait_recv()
    load_own.wait()
    tasks.extend([functools.partial(store_slab, number) for number in range(features // slab)])
    ending = 64
    tasks.extend([functools.partial(store_end, first, min(ending, quarter - first)) for first in range(0, quarter, ending)])
    tasks.append(functools.partial(w_end, 0))
    for step in range(2, hops):
        for part in range(4):
            dq_step(1, step, part)
            fill()
        w_step(step, 1)
        fill()
    fill(len(tasks))
    for part in range(4):
        dq_end(1, part)
    w_end(1)
    for copy in sends:
        copy.wait_send()


def query_plan(queries, gate_pre, cotangent, store, store_gain, w_key, w_value, owners, slots):
    n = lax.axis_size("st")
    tp = lax.axis_size("tp")
    blocks, per_block = owners.shape
    tok_rows, width = queries.shape
    heads = width // HD
    block_len = tok_rows // blocks
    rows_dev, features = store.shape
    passages = rows_dev // PLEN
    quarter = rows_dev // tp
    total = n * blocks
    hops = n // 2
    feats = features // n
    blocked = [one.reshape(blocks, block_len, width) for one in (queries, gate_pre, cotangent)]
    vmem = pl.BlockSpec(memory_space=pltpu.VMEM)
    anywhere = pl.BlockSpec(memory_space=pltpu.HBM)
    half, wide = jnp.bfloat16, jnp.float32
    dma = pltpu.SemaphoreType.DMA

    def per_head(shape, kind):
        return [pltpu.VMEM(shape, kind) for _ in range(heads)]

    return pl.pallas_call(
        functools.partial(whole_kernel, n, tp),
        out_shape=(
            jax.ShapeDtypeStruct((tok_rows, width), wide),
            jax.ShapeDtypeStruct((quarter, features), wide),
            jax.ShapeDtypeStruct((feats, width), wide),
        ),
        in_specs=[anywhere] * 9,
        out_specs=(vmem,) * 3,
        scratch_shapes=[
            pltpu.VMEM((1, features), wide),
            pltpu.VMEM((per_block, blocks), jnp.int32),
            pltpu.VMEM((per_block, blocks), jnp.int32),
            pltpu.VMEM((8, 128), wide),
            pltpu.VMEM((blocks, 128), jnp.int32),
            per_head((total, block_len, HD), half),
            per_head((total, block_len, HD), half),
            pltpu.VMEM((n, blocks, 128), jnp.int32),
            pltpu.VMEM((blocks, block_len, width), half),
            pltpu.VMEM((blocks, block_len, width), half),
            pltpu.VMEM((2, CHUNK, features), half),
            pltpu.VMEM((quarter, features), half),
            pltpu.VMEM((rows_dev, features), half),
            pltpu.VMEM((features, 2 * tp * width), half),
            per_head((passages, PLEN, HD), half),
            per_head((passages, PLEN, HD), half),
            pltpu.VMEM((8, 128), jnp.int32),
            pltpu.SMEM((8, 128), jnp.int32),
            per_head((n + 1, 2, blocks, block_len), wide),
            per_head((n, 2, blocks, block_len), wide),
            per_head((total + 4, 2, block_len), wide),
            per_head((total, block_len, HD), half),
            pltpu.VMEM((total, PLEN, HD), half),
            pltpu.VMEM((total, PLEN, HD), half),
            per_head((rows_dev, HD), half),
            per_head((rows_dev, HD), half),
            pltpu.VMEM((heads, HD, rows_dev), half),
            pltpu.VMEM((quarter, 2 * tp * width), half),
            per_head((blocks, block_len, HD), half),
            per_head((2, hops, blocks, block_len, HD), half),
            pltpu.VMEM((heads, HD, feats), half),
            pltpu.VMEM((2, hops, heads, HD, feats), half),
            dma((heads + 8,)),
            dma((2,)),
            dma((heads, 2, hops, 4)),
            dma((heads, 2, hops, 4)),
            dma((n,)),
            dma((n,)),
            dma((heads, 2, n)),
            dma((heads, 2, n)),
            dma((heads, 2, hops, 4)),
            dma((heads, 2, hops, 4)),
            dma((2, hops, heads)),
            dma((2, hops, heads)),
            dma((heads, 2, tp)),
            dma((heads, 2, tp)),
            dma((2, 3)),
            dma((2, 3)),
            dma((1,)),
        ],
        cost_estimate=pl.CostEstimate(flops=2 * 10**10, bytes_accessed=3 * 10**7, transcendentals=0),
        compiler_params=pltpu.CompilerParams(collective_id=0, has_side_effects=True, vmem_limit_bytes=VMEM_LIMIT),
        name="whole",
    )(*[pltpu.with_memory_space_constraint(one, pltpu.HBM) for one in (*blocked, store, w_key, w_value, store_gain[None], owners.T, slots.T)])


def fits(queries, store, owners):
    n, tp = lax.axis_size("st"), lax.axis_size("tp")
    blocks = owners.shape[0]
    block_len = queries.shape[0] // blocks
    slot_cap = (2 * owners.size + n - 1) // n
    return (
        n % 2 == 0 and n >= 8 and tp == 4 and blocks == 8 and n * blocks <= 128
        and block_len == 128 and queries.shape[1] == 2 * HD
        and store.shape[0] % (tp * CHUNK // 2) == 0 and store.shape[0] % 256 == 0
        and store.shape[0] // PLEN <= 128 and store.shape[1] % (256 * n) == 0
        and 8 * slot_cap * PLEN >= 3 * queries.shape[0]
    )


def local(*arrays):
    if fits(arrays[0], arrays[3], arrays[7]):
        return query_plan(*arrays)
    return passage_plan(*arrays)


def solution(mesh):
    placed = (
        P("st", "tp"),
        P("st", "tp"),
        P("st", "tp"),
        P("st", None),
        P(),
        P(None, "tp"),
        P(None, "tp"),
        P("st", None),
        P("st", None),
    )
    return jax.shard_map(
        local,
        mesh=mesh,
        in_specs=placed,
        out_specs=(P("st", "tp"), P(("st", "tp"), None), P("st", "tp")),
        check_vma=False,
    )
```

```python
import functools

import jax
import jax.numpy as jnp
from jax import lax
from jax.experimental import pallas as pl
from jax.experimental.pallas import tpu as pltpu
from jax.sharding import PartitionSpec as P

HD = 128
PLEN = 64


EPS = 1e-06


def row_scale(store_rows):
    return lax.rsqrt(jnp.mean(store_rows * store_rows, axis=-1, keepdims=True) + EPS)


def contract(left, right):
    return lax.dot_general(
        left, right, (((1,), (1,)), ((), ())), preferred_element_type=jnp.float32
    )


def passage_plan(queries, gate_pre, cotangent, store, store_gain, w_key, w_value, owners, slots):
    st_size = lax.axis_size("st")
    tp_size = lax.axis_size("tp")
    blocks, per_block = owners.shape
    tok_rows, local_width = queries.shape
    head_dim = HD
    local_heads = local_width // head_dim
    block_len = tok_rows // blocks
    passage_len = PLEN
    rows_dev = store.shape[0]
    passages = rows_dev // passage_len
    slot_count = blocks * per_block
    slot_cap = (2 * slot_count + st_size - 1) // st_size
    store_rows = store.astype(jnp.float32)
    row_inverse = row_scale(store_rows)
    normed = (store_rows * row_inverse * store_gain).astype(jnp.bfloat16)
    key_table = jnp.dot(normed, w_key, preferred_element_type=jnp.float32).astype(jnp.bfloat16)
    value_table = jnp.dot(normed, w_value, preferred_element_type=jnp.float32).astype(jnp.bfloat16)
    key_table = key_table.reshape(passages, passage_len, local_width)
    value_table = value_table.reshape(passages, passage_len, local_width)
    owner_flat = owners.reshape(slot_count)
    slot_flat = slots.reshape(slot_count)
    slot_order = jnp.arange(slot_count, dtype=jnp.int32)
    earlier_same = (owner_flat[:, None] == owner_flat[None, :]) & (
        slot_order[None, :] < slot_order[:, None]
    )
    slot_rank = jnp.sum(earlier_same.astype(jnp.int32), axis=1)
    position = owner_flat * slot_cap + slot_rank
    places = jnp.arange(st_size * slot_cap, dtype=jnp.int32)
    slot_hits = position[:, None] == places[None, :]
    requests = jnp.sum(jnp.where(slot_hits, slot_flat[:, None], 0), axis=0)
    requests = requests.reshape(st_size, slot_cap)
    asked_ids = lax.all_to_all(requests, "st", split_axis=0, concat_axis=0, tiled=True)
    asked_flat = asked_ids.reshape(-1)
    shape_out = asked_ids.shape + (passage_len, local_width)
    picked_keys = jnp.take(key_table, asked_flat, axis=0).reshape(shape_out)
    picked_values = jnp.take(value_table, asked_flat, axis=0).reshape(shape_out)
    sent_keys = lax.all_to_all(picked_keys, "st", split_axis=0, concat_axis=0, tiled=True)
    sent_values = lax.all_to_all(picked_values, "st", split_axis=0, concat_axis=0, tiled=True)
    got_keys, got_values, asked_ids = (sent_keys, sent_values, asked_ids)
    span = per_block * passage_len
    mine_keys = jnp.take(
        got_keys.reshape(st_size * slot_cap, passage_len, local_width), position, axis=0
    )
    mine_values = jnp.take(
        got_values.reshape(st_size * slot_cap, passage_len, local_width), position, axis=0
    )
    mine_keys = mine_keys.reshape(blocks, span, local_heads, head_dim)
    mine_values = mine_values.reshape(blocks, span, local_heads, head_dim)
    score_scale = head_dim ** (-0.5)
    query_blocks = queries.reshape(blocks, block_len, local_heads, head_dim)
    gate_open = jax.nn.sigmoid(gate_pre.astype(jnp.float32))
    grad_in = (gate_open * cotangent.astype(jnp.float32)).astype(jnp.bfloat16)
    grad_in = grad_in.reshape(blocks, block_len, local_heads, head_dim)
    scores = (
        jnp.einsum("bqhd,bkhd->bhqk", query_blocks, mine_keys, preferred_element_type=jnp.float32)
        * score_scale
    )
    shifted = scores - jnp.max(scores, axis=-1, keepdims=True)
    weights = jnp.exp(shifted)
    weights = weights / jnp.sum(weights, axis=-1, keepdims=True)
    weights_half = weights.astype(jnp.bfloat16)
    attended = jnp.einsum(
        "bhqk,bkhd->bqhd", weights_half, mine_values, preferred_element_type=jnp.float32
    )
    row_delta = jnp.sum(grad_in.astype(jnp.float32) * attended, axis=-1)
    grad_weights = jnp.einsum(
        "bqhd,bkhd->bhqk", grad_in, mine_values, preferred_element_type=jnp.float32
    )
    grad_scores = weights * (grad_weights - jnp.transpose(row_delta, (0, 2, 1))[..., None])
    grad_half = grad_scores.astype(jnp.bfloat16)
    grad_queries = (
        jnp.einsum("bhqk,bkhd->bqhd", grad_half, mine_keys, preferred_element_type=jnp.float32)
        * score_scale
    )
    grad_queries = grad_queries.reshape(tok_rows, local_width)
    grad_keys = (
        jnp.einsum("bhqk,bqhd->bkhd", grad_half, query_blocks, preferred_element_type=jnp.float32)
        * score_scale
    )
    grad_values = jnp.einsum(
        "bhqk,bqhd->bkhd", weights_half, grad_in, preferred_element_type=jnp.float32
    )
    grad_keys = grad_keys.reshape(slot_count, passage_len, local_width)
    grad_values = grad_values.reshape(slot_count, passage_len, local_width)
    empty_slots = jnp.zeros((st_size * slot_cap, passage_len, local_width), jnp.bfloat16)
    outgoing_keys = empty_slots.at[position].set(grad_keys.astype(jnp.bfloat16))
    outgoing_values = empty_slots.at[position].set(grad_values.astype(jnp.bfloat16))
    back_keys, back_values = (
        lax.all_to_all(outgoing_keys, "st", split_axis=0, concat_axis=0, tiled=True),
        lax.all_to_all(outgoing_values, "st", split_axis=0, concat_axis=0, tiled=True),
    )
    asked_flat = asked_ids.reshape(-1)
    owner_pick = (asked_flat[None, :] == jnp.arange(passages, dtype=jnp.int32)[:, None]).astype(
        jnp.bfloat16
    )
    passage_keys = jnp.dot(
        owner_pick,
        back_keys.reshape(st_size * slot_cap, passage_len * local_width),
        preferred_element_type=jnp.float32,
    )
    passage_values = jnp.dot(
        owner_pick,
        back_values.reshape(st_size * slot_cap, passage_len * local_width),
        preferred_element_type=jnp.float32,
    )
    passage_keys = passage_keys.astype(jnp.bfloat16).reshape(rows_dev, local_width)
    passage_values = passage_values.astype(jnp.bfloat16).reshape(rows_dev, local_width)
    weight_terms = lax.dot_general(
        normed, passage_values, (((0,), (0,)), ((), ())), preferred_element_type=jnp.float32
    )
    grad_w_value = lax.psum_scatter(weight_terms, "st", scatter_dimension=0, tiled=True)
    quarter = rows_dev // tp_size
    whole_key, whole_value = (
        lax.all_gather(w_key, "tp", axis=1, tiled=True),
        lax.all_gather(w_value, "tp", axis=1, tiled=True),
    )
    own_keys, own_values = (
        lax.all_to_all(passage_keys, "tp", split_axis=0, concat_axis=1, tiled=True),
        lax.all_to_all(passage_values, "tp", split_axis=0, concat_axis=1, tiled=True),
    )
    grad_normed = contract(own_keys, whole_key) + contract(own_values, whole_value)
    first_row = lax.axis_index("tp") * quarter
    own_rows = lax.dynamic_slice_in_dim(store_rows, first_row, quarter, 0)
    own_inverse = lax.dynamic_slice_in_dim(row_inverse, first_row, quarter, 0)
    unit_rows = own_rows * own_inverse
    grad_unit = grad_normed * store_gain
    grad_store = own_inverse * (
        grad_unit - unit_rows * jnp.mean(grad_unit * unit_rows, axis=-1, keepdims=True)
    )
    return (grad_queries, grad_store, grad_w_value)

FAR = 1e30
MESH = pl.DeviceIdType.MESH
NT = (((1,), (1,)), ((), ()))
TN = (((0,), (0,)), ((), ()))
CHUNK = 128
VMEM_LIMIT = 45 << 20


def place_of(index, n):
    odd = index % 2
    return (1 - odd) * (index // 2) + odd * (n - 1 - index // 2)


def index_at(place, n):
    place = (place + 2 * n) % n
    back = place // (n // 2)
    return (1 - back) * (2 * place) + back * (2 * (n - 1 - place) + 1)


def dot(left, right, dims=(((1,), (0,)), ((), ()))):
    return lax.dot_general(left, right, dims, preferred_element_type=jnp.float32)


def as_float(flag):
    return jnp.where(flag, jnp.float32(1.0), jnp.float32(0.0))


def rows_of_table(named, first, passages):
    total = named.shape[0]
    held = (named - first).astype(jnp.float32)
    inside = (held >= 0.0) & (held < passages)
    col = jnp.max(jnp.where(inside, held, -1.0), axis=1, keepdims=True)
    spot_col = lax.broadcasted_iota(jnp.int32, (128, 128), 0).astype(jnp.float32)
    spot_row = lax.broadcasted_iota(jnp.int32, (128, 128), 1).astype(jnp.float32)
    wide = jnp.broadcast_to(col, (total, 128))
    if total < 128:
        wide = jnp.concatenate([wide, jnp.full((128 - total, 128), 1000.0, jnp.float32)], axis=0)
    ids_row = wide.T
    key_col = wide * 128.0 + spot_col
    key_row = key_col.T
    rank_col = jnp.sum(as_float(key_row < key_col), axis=1, keepdims=True)
    rank_row = jnp.sum(as_float(key_col < key_row), axis=0, keepdims=True)
    order_row = jnp.sum(as_float(rank_col == spot_row) * spot_col, axis=0, keepdims=True)
    last_row = jnp.sum(as_float(wide <= spot_row), axis=0, keepdims=True) - 1.0
    has_row = jnp.max(as_float(wide == spot_row), axis=0, keepdims=True)
    rows = [ids_row[:1], rank_row, order_row, jnp.maximum(last_row, 0.0), has_row, jnp.zeros((3, 128), jnp.float32)]
    return jnp.concatenate(rows, axis=0).astype(jnp.int32)


IDS, RANK, ORDER, LAST, HAS = range(5)


def whole_kernel(n, tp, q_hbm, gate_hbm, cot_hbm, x_hbm, wk_hbm, wv_hbm, gain_hbm, owners_hbm, slots_hbm,
                 dq_ref, gs_ref, gw_ref,
                 gain_ref, owners_buf, slots_buf, flat, named_ref, q_all, g_all, i_all, gate_buf, cot_buf, x_buf, own_x, normed, whole, kt, vt,
                 tab_buf, tab, stats, got, joined, dq_sorted, tk, tv, pk, pv, pv_flip, own_kv,
                 dq_send, dq_recv, w_send, w_recv,
                 in_sem, x_sem, g_send, g_recv, i_send, i_recv, j_send, j_recv,
                 s_send, s_recv, ws_send, ws_recv, p_send, p_recv, t_send, t_recv, tab_sem):
    me, mine = lax.axis_index("st"), lax.axis_index("tp")
    place = place_of(me, n)
    right, left = index_at(place + 1, n), index_at(place - 1, n)
    hops = n // 2
    heads = len(q_all)
    total, block_len = q_all[0].shape[:2]
    blocks = total // n
    passages = kt[0].shape[0]
    rows_dev, features = normed.shape
    quarter = rows_dev // tp
    width = heads * HD
    feats = features // n
    scale = HD ** (-0.5)
    sibling = mine + 1 - 2 * (mine % 2)
    across = (mine + tp // 2) % tp
    half = blocks // 2

    barrier = pltpu.get_barrier_semaphore()
    for away in range(1, n):
        pl.semaphore_signal(barrier, inc=1, device_id={"st": (me + away) % n}, device_id_type=MESH)
    for away in range(1, tp):
        pl.semaphore_signal(barrier, inc=1, device_id={"tp": (mine + away) % tp}, device_id_type=MESH)

    def columns(owner, value):
        return pl.ds(pl.multiple_of(value * tp * width + owner * width, 128), width)

    loads = []
    for head in range(heads):
        loads.append(pltpu.make_async_copy(q_hbm.at[:, :, pl.ds(head * HD, HD)], q_all[head].at[pl.ds(me * blocks, blocks)], in_sem.at[head]))
    load_gate = pltpu.make_async_copy(gate_hbm, gate_buf, in_sem.at[heads])
    load_cot = pltpu.make_async_copy(cot_hbm, cot_buf, in_sem.at[heads + 1])
    load_w = [pltpu.make_async_copy(ref, whole.at[:, columns(mine, number)], in_sem.at[heads + 2 + number]) for number, ref in enumerate((wk_hbm, wv_hbm))]
    load_small = [pltpu.make_async_copy(src, dst, in_sem.at[heads + 5 + number]) for number, (src, dst) in enumerate(((owners_hbm, owners_buf), (slots_hbm, slots_buf), (gain_hbm, gain_ref)))]
    load_own = pltpu.make_async_copy(x_hbm.at[pl.ds(pl.multiple_of(mine * quarter, 16), quarter)], own_x, in_sem.at[heads + 4])

    def load_x(chunk):
        return pltpu.make_async_copy(x_hbm.at[pl.ds(chunk * CHUNK, CHUNK)], x_buf.at[chunk % 2], x_sem.at[chunk % 2])

    for copy in load_small[:2] + loads + [load_gate, load_cot] + load_w + load_small[2:] + [load_x(0), load_own]:
        copy.start()

    def begin(copy):
        copy.start()

    def remote(src, dst, send_sem, recv_sem, **to):
        return pltpu.make_async_remote_copy(src_ref=src, dst_ref=dst, send_sem=send_sem, recv_sem=recv_sem, device_id=to, device_id_type=MESH)

    def whole_batch(ref, send_sem, recv_sem):
        return remote(ref, ref, send_sem, recv_sem, st=right)

    parts = ((0, 0), (0, 1), (1, 0), (1, 1))

    def gather_piece(head, side, step, part):
        number, which = parts[part]
        ref = (q_all, g_all)[number][head]
        origin = index_at(place - step, n) if side == 0 else index_at(place + step, n)
        at = ref.at[pl.ds(origin * blocks + which * half, half)]
        return remote(at, at, g_send.at[head, number], g_recv.at[head, side, step, part], st=right if side == 0 else left)

    def goes(side, step, part):
        return step < hops - 1 or parts[part][1] == side

    def ids_piece(away):
        return remote(named_ref, i_all.at[me], i_send.at[0], i_recv.at[0], st=(me + away) % n)

    def weight_piece(number, way):
        owner = mine if way < 2 else across
        at = whole.at[:, columns(owner, number)]
        return remote(at, at, t_send.at[number], t_recv.at[number, way], tp=across if way == 1 else sibling)

    def make_grad_in():
        load_gate.wait()
        load_cot.wait()

        @pl.loop(0, blocks)
        def _(block):
            for head in range(heads):
                cols = pl.ds(head * HD, HD)
                opened = jax.nn.sigmoid(gate_buf[block, :, cols].astype(jnp.float32))
                g_all[head][me * blocks + block] = (opened * cot_buf[block, :, cols].astype(jnp.float32)).astype(jnp.bfloat16)

    def project(chunk):
        if (chunk + 1) * CHUNK < rows_dev:
            load_x(chunk + 1).start()
        load_x(chunk).wait()
        rows = pl.ds(chunk * CHUNK, CHUNK)
        wide = x_buf[chunk % 2].astype(jnp.float32)
        ready = (wide * row_scale(wide) * gain_ref[...]).astype(jnp.bfloat16)
        normed[rows] = ready
        per = CHUNK // PLEN
        for number, table in enumerate((kt, vt)):
            out = dot(ready, whole[:, columns(mine, number)]).astype(jnp.bfloat16)
            for head in range(heads):
                table[head][pl.ds(chunk * per, per)] = out[:, head * HD:(head + 1) * HD].reshape(per, PLEN, HD)

    def make_table():
        whole_batch(i_all.at[pl.ds(0, n - 1)], i_send.at[0], i_recv.at[0]).wait_recv()
        tab_buf[...] = rows_of_table(i_all[...].reshape(total, 128), me * passages, passages)
        copy = pltpu.make_async_copy(tab_buf, tab, tab_sem.at[0])
        copy.start()
        copy.wait()

    def make_stats(head, origin):
        for first in range(0, blocks, 4):
            count = min(4, blocks - first)
            spots = [origin * blocks + first + lane for lane in range(count)]
            ids = [jnp.minimum(tab[IDS, spot], passages - 1) for spot in spots]
            scores = [dot(kt[head][jnp.maximum(one, 0)], q_all[head][spot], NT) * scale for one, spot in zip(ids, spots)]
            grads = [dot(vt[head][jnp.maximum(one, 0)], g_all[head][spot], NT) for one, spot in zip(ids, spots)]
            tops = [jnp.max(one, axis=0, keepdims=True) for one in scores]
            raised = [jnp.exp(one - top) for one, top in zip(scores, tops)]
            totals = [jnp.sum(one, axis=0, keepdims=True) for one in raised]
            means = [jnp.sum(one * two, axis=0, keepdims=True) / three for one, two, three in zip(raised, grads, totals)]
            for lane in range(count):
                dead = jnp.minimum(ids[lane], 0).astype(jnp.float32) * FAR
                stats[head][origin, 0, pl.ds(first + lane, 1)] = tops[lane] + jnp.log(totals[lane]) + dead
                stats[head][origin, 1, pl.ds(first + lane, 1)] = means[lane]

    def join_piece(head, phase, away):
        peer = (me + away) % n
        at = joined[head].at[pl.ds(me * blocks, blocks)]
        return remote(
            stats[head].at[peer] if phase == 0 else at,
            got[head].at[me] if phase == 0 else at,
            j_send.at[head, phase], j_recv.at[head, phase], st=peer)

    def join_batch(head, phase):
        ref = got[head].at[pl.ds(0, n - 1)] if phase == 0 else joined[head].at[pl.ds(0, (n - 1) * blocks)]
        return whole_batch(ref, j_send.at[head, phase], j_recv.at[head, phase])

    def join_first(head):
        for away in range(1, n):
            begin(join_piece(head, 0, away))
        got[head][me] = stats[head][me]

    def join_second(head):
        join_batch(head, 0).wait_recv()
        logs = [got[head][owner, 0] for owner in range(n)]
        top = functools.reduce(jnp.maximum, logs)
        shares = [jnp.exp(one - top) for one in logs]
        whole_sum = sum(shares)
        final = top + jnp.log(whole_sum)
        mean = sum(share * got[head][owner, 1] for owner, share in enumerate(shares)) / whole_sum
        for block in range(blocks):
            joined[head][me * blocks + block, 0:1] = final[block:block + 1]
            joined[head][me * blocks + block, 1:2] = mean[block:block + 1]
        for away in range(1, n):
            begin(join_piece(head, 1, away))

    def join_last(head):
        join_batch(head, 1).wait_recv()

    lanes = 4

    def make_grads(head, begin_turn, end_turn, carry):
        def turn_body(turn, carry):
            acc_k, acc_v, past = carry
            spots = [jnp.clip(tab[ORDER, turn * lanes + lane], 0, total - 1) for lane in range(lanes)]
            ids = [jnp.minimum(tab[IDS, spot], passages - 1) for spot in spots]
            keys = [kt[head][jnp.maximum(one, 0)] for one in ids]
            queries = [q_all[head][spot] for spot in spots]
            givens = [g_all[head][spot] for spot in spots]
            scores = [dot(key, query, NT) * scale for key, query in zip(keys, queries)]
            grads = [dot(vt[head][jnp.maximum(one, 0)], given, NT) for one, given in zip(ids, givens)]
            weights, halves = [], []
            for one, spot, score, grad in zip(ids, spots, scores, grads):
                logs = joined[head][spot, 0:1] - jnp.minimum(one, 0).astype(jnp.float32) * FAR
                weight = jnp.exp(score - logs)
                halves.append((weight * (grad - joined[head][spot, 1:2])).astype(jnp.bfloat16))
                weights.append(weight.astype(jnp.bfloat16))
            term_k = [dot(one, query) for one, query in zip(halves, queries)]
            term_v = [dot(one, given) for one, given in zip(weights, givens)]
            steps = [dot(one, key, TN) for one, key in zip(halves, keys)]
            for lane in range(lanes):
                keep = as_float(ids[lane] == past)
                past = ids[lane]
                acc_k = acc_k * keep + term_k[lane]
                acc_v = acc_v * keep + term_v[lane]
                at = turn * lanes + lane
                tk[at] = (acc_k * scale).astype(jnp.bfloat16)
                tv[at] = acc_v.astype(jnp.bfloat16)
                dq_sorted[head][at] = (steps[lane] * scale).astype(jnp.bfloat16)
            return acc_k, acc_v, past

        return lax.fori_loop(begin_turn, end_turn, turn_body, carry)

    blank = (jnp.zeros((PLEN, HD), jnp.float32), jnp.zeros((PLEN, HD), jnp.float32), jnp.int32(-2))
    turns = total // lanes

    def pick(head):
        @pl.loop(0, passages)
        def _(passage):
            last = jnp.clip(tab[LAST, passage], 0, total - 1)
            has = tab[HAS, passage].astype(jnp.float32)
            rows = pl.ds(pl.multiple_of(passage * PLEN, PLEN), PLEN)
            pk[head][rows] = (tk[last].astype(jnp.float32) * has).astype(jnp.bfloat16)
            pv[head][rows] = (tv[last].astype(jnp.float32) * has).astype(jnp.bfloat16)

    def own_columns(owner, head, number):
        return pl.ds(pl.multiple_of(number * tp * width + owner * width + head * HD, 128), HD)

    def passage_piece(head, number, away):
        peer = (mine + away) % tp
        rows = pl.ds(pl.multiple_of(peer * quarter, 16), quarter)
        return remote((pk, pv)[number][head].at[rows], own_kv.at[:, own_columns(mine, head, number)],
                      p_send.at[head, number], p_recv.at[head, number], tp=peer)

    def passage_batch(head, number):
        ref = (pk, pv)[number][head].at[pl.ds(0, (tp - 1) * quarter)]
        return remote(ref, ref, p_send.at[head, number], p_recv.at[head, number], tp=sibling)

    def share(head):
        for number in range(2):
            for away in range(1, tp):
                begin(passage_piece(head, number, away))
            rows = pl.ds(pl.multiple_of(mine * quarter, 16), quarter)
            own_kv[:, own_columns(mine, head, number)] = (pk, pv)[number][head][rows]

    dq_parts = ((0, 0), (half, 1), (half // 2, 0), (half + half // 2, 1))
    dq_count = half // 2

    def used(side, step, part):
        return step > 0 or dq_parts[part][1] == side

    def dq_piece(head, side, step, part):
        at = pl.ds(dq_parts[part][0], dq_count)
        src = dq_recv[head].at[side, step - 1, at] if step > 0 else dq_send[head].at[at]
        return remote(src, dq_recv[head].at[side, step, at],
                      s_send.at[head], s_recv.at[head, side, step, part], st=right if side == 0 else left)

    def dest_of(side, step):
        distance = hops - step
        return index_at(place + distance, n) if side == 0 else index_at(place - distance, n)

    def dq_step(head, step, part):
        for side in range(2):
            if not used(side, step, part):
                continue
            dest = dest_of(side, step)
            arrived = step > 0 and used(side, step - 1, part)
            if arrived:
                dq_piece(head, side, step - 1, part).wait_recv()
            for lane in range(dq_count):
                block = dq_parts[part][0] + lane
                value = dq_sorted[head][jnp.clip(tab[RANK, dest * blocks + block], 0, total - 1)]
                if arrived:
                    value = (value.astype(jnp.float32) + dq_recv[head][side, step - 1, block].astype(jnp.float32)).astype(jnp.bfloat16)
                if step > 0:
                    dq_recv[head][side, step - 1, block] = value
                else:
                    dq_send[head][block] = value
            begin(dq_piece(head, side, step, part))

    def dq_end(head, part):
        for side in range(2):
            dq_piece(head, side, hops - 1, part).wait_recv()
        for lane in range(dq_count):
            block = dq_parts[part][0] + lane
            value = dq_sorted[head][jnp.clip(tab[RANK, me * blocks + block], 0, total - 1)].astype(jnp.float32)
            for side in range(2):
                value = value + dq_recv[head][side, hops - 1, block].astype(jnp.float32)
            dq_ref[pl.ds(block * block_len, block_len), pl.ds(head * HD, HD)] = value

    def w_at(side, step, part):
        return (side * hops + step) * heads + part

    def w_piece(side, step, part):
        src = w_recv.at[w_at(side, step - 1, part)] if step > 0 else w_send.at[part]
        return remote(src, w_recv.at[w_at(side, step, part)],
                      ws_send.at[0], ws_recv.at[side, step, part], st=right if side == 0 else left)

    def w_term(dest, part):
        return dot(pv_flip[part], normed[:, pl.ds(pl.multiple_of(dest * feats, 128), feats)])

    def w_used(side, step, part):
        return step > 0 or part % 2 == side

    def w_step(step, part):
        for side in range(2):
            if not w_used(side, step, part):
                continue
            value = w_term(dest_of(side, step), part)
            if step > 0 and w_used(side, step - 1, part):
                w_piece(side, step - 1, part).wait_recv()
                value = value + w_recv[w_at(side, step - 1, part)].astype(jnp.float32)
            if step > 0:
                w_recv[w_at(side, step - 1, part)] = value.astype(jnp.bfloat16)
            else:
                w_send[part] = value.astype(jnp.bfloat16)
            begin(w_piece(side, step, part))

    def w_end(part):
        value = w_term(me, part)
        for side in range(2):
            w_piece(side, hops - 1, part).wait_recv()
            value = value + w_recv[w_at(side, hops - 1, part)].astype(jnp.float32)
        gw_ref[:, pl.ds(part * HD, HD)] = value.T

    def flip(head):
        for first in range(0, rows_dev, 256):
            pv_flip[head, :, pl.ds(first, 256)] = pv[head][pl.ds(first, 256)].astype(jnp.float32).T.astype(jnp.bfloat16)

    slab = 256

    def store_slab(number):
        cols = pl.ds(number * slab, slab)
        gs_ref[:, cols] = dot(own_kv[...], whole[cols], NT) * gain_ref[:, cols]

    def store_end(first, count):
        rows = pl.ds(first, count)
        wide = own_x[rows].astype(jnp.float32)
        inverse = row_scale(wide)
        unit = wide * inverse
        value = gs_ref[rows]
        gs_ref[rows] = inverse * (value - unit * jnp.mean(value * unit, axis=-1, keepdims=True))

    for copy in load_small[:2]:
        copy.wait()
    per_block = owners_buf.shape[0]
    flat[...] = jnp.full(flat.shape, -1.0, jnp.float32)
    flat[pl.ds(0, per_block), pl.ds(0, blocks)] = (owners_buf[...] * passages + slots_buf[...]).astype(jnp.float32)
    named_ref[...] = jnp.full(named_ref.shape, -1, jnp.int32)
    named_ref[:, pl.ds(0, 8)] = flat[...].T[:blocks].astype(jnp.int32)
    loads[0].wait()
    pl.semaphore_wait(barrier, n - 1 + tp - 1)
    for part in range(2):
        for side in range(2):
            begin(gather_piece(0, side, 0, part))
    make_grad_in()
    for part in range(2, 4):
        for side in range(2):
            begin(gather_piece(0, side, 0, part))
    for away in range(1, n):
        begin(ids_piece(away))
    i_all[me] = named_ref[...]
    for copy in load_w:
        copy.wait()
    for number in range(2):
        begin(weight_piece(number, 1))
        begin(weight_piece(number, 0))
    load_small[2].wait()
    for copy in loads[1:]:
        copy.wait()

    tasks = [functools.partial(project, chunk) for chunk in range(rows_dev // CHUNK)]
    tasks.append(make_table)
    tasks.append(functools.partial(make_stats, 0, me))

    def idle():
        pass

    def fill(count=1):
        for _ in range(count):
            if tasks:
                tasks.pop(0)()

    def both(head, step):
        def run():
            make_stats(head, index_at(place - step, n))
            make_stats(head, index_at(place + step, n))
        return run

    state = {0: blank, 1: blank}

    def grads_task(head, first, last):
        def run():
            state[head] = make_grads(head, first, last, state[head])
        return run

    def grad_tasks(head, pieces):
        edges = [turns * piece // pieces for piece in range(pieces + 1)]
        return [grads_task(head, edges[piece], edges[piece + 1]) for piece in range(pieces)]

    def gather_step(head, step):
        for part in range(4):
            for side in range(2):
                if goes(side, step, part):
                    if step > 0:
                        gather_piece(head, side, step - 1, part).wait_recv()
                    begin(gather_piece(head, side, step, part))
            fill()

    def gather_rest(head, first):
        if first:
            for part in range(4):
                for side in range(2):
                    if not goes(side, hops - 1, part):
                        gather_piece(head, side, hops - 2, part).wait_recv()
        else:
            for part in range(4):
                gather_piece(head, parts[part][1], hops - 1, part).wait_recv()

    def forward_weights():
        for number in range(2):
            weight_piece(number, 1).wait_recv()
            begin(weight_piece(number, 2))

    for step in range(1, hops):
        gather_step(0, step)
        if step < hops - 1:
            tasks.append(both(0, step))
    for part in range(4):
        for side in range(2):
            begin(gather_piece(1, side, 0, part))
        fill()
    gather_rest(0, True)
    tasks.append(both(0, hops - 1))
    fill(len(tasks))
    gather_rest(0, False)
    make_stats(0, index_at(place + hops, n))
    join_first(0)
    tasks.extend([functools.partial(make_stats, 1, me), idle, functools.partial(join_second, 0), forward_weights])
    gather_step(1, 1)
    tasks.extend([both(1, 1), idle, idle, functools.partial(join_last, 0)])
    gather_step(1, 2)
    tasks.extend(grad_tasks(0, 4))
    tasks.extend([functools.partial(pick, 0), functools.partial(share, 0), functools.partial(flip, 0)])
    for step in range(3, hops):
        gather_step(1, step)
    fill(len(tasks))
    for part in range(4):
        dq_step(0, 0, part)
    for step in range(2, hops - 1):
        both(1, step)()
    gather_rest(1, True)
    both(1, hops - 1)()
    gather_rest(1, False)
    make_stats(1, index_at(place + hops, n))
    join_first(1)
    for part in range(2):
        dq_step(0, 1, part)
    join_second(1)
    for part in range(2, 4):
        dq_step(0, 1, part)
    w_step(0, 0)
    for part in range(2):
        dq_step(0, 2, part)
    join_last(1)
    tasks.extend(grad_tasks(1, 8))
    for part in range(2, 4):
        dq_step(0, 2, part)
        fill()
    w_step(1, 0)
    fill()
    for step in range(3, hops):
        for part in range(4):
            dq_step(0, step, part)
            fill()
    fill(len(tasks))
    for part in range(4):
        dq_step(1, 0, part)
    w_step(2, 0)
    pick(1)
    share(1)
    flip(1)
    w_step(0, 1)
    for part in range(4):
        dq_end(0, part)
    for part in range(4):
        dq_step(1, 1, part)
    w_step(3, 0)
    w_step(1, 1)
    for number in range(2):
        for way in (0, 2):
            weight_piece(number, way).wait_recv()
    for head in range(heads):
        for number in range(2):
            passage_batch(head, number).wait_recv()
    load_own.wait()
    tasks.extend([functools.partial(store_slab, number) for number in range(features // slab)])
    ending = 64
    tasks.extend([functools.partial(store_end, first, min(ending, quarter - first)) for first in range(0, quarter, ending)])
    tasks.append(functools.partial(w_end, 0))
    for step in range(2, hops):
        for part in range(4):
            dq_step(1, step, part)
            fill()
        w_step(step, 1)
        fill()
    fill(len(tasks))
    for part in range(4):
        dq_end(1, part)
    w_end(1)
    for head in range(heads):
        for number in range(2):
            ref = (q_all, g_all)[number][head].at[pl.ds(0, (n - 1) * blocks)]
            whole_batch(ref, g_send.at[head, number], g_recv.at[head, 0, 0, 0]).wait_send()
            join_batch(head, number).wait_send()
            passage_batch(head, number).wait_send()
        whole_batch(dq_sorted[head].at[pl.ds(0, (n - 1) * blocks)], s_send.at[head], s_recv.at[head, 0, 0, 0]).wait_send()
    for number in range(2):
        ref = whole.at[:, pl.ds(0, (tp - 1) * width)]
        remote(ref, ref, t_send.at[number], t_recv.at[number, 0], tp=sibling).wait_send()
    whole_batch(w_recv.at[pl.ds(0, (n - 1) * heads)], ws_send.at[0], ws_recv.at[0, 0, 0]).wait_send()
    whole_batch(i_all.at[pl.ds(0, n - 1)], i_send.at[0], i_recv.at[0]).wait_send()


def query_plan(queries, gate_pre, cotangent, store, store_gain, w_key, w_value, owners, slots):
    n = lax.axis_size("st")
    tp = lax.axis_size("tp")
    blocks, per_block = owners.shape
    tok_rows, width = queries.shape
    heads = width // HD
    block_len = tok_rows // blocks
    rows_dev, features = store.shape
    passages = rows_dev // PLEN
    quarter = rows_dev // tp
    total = n * blocks
    hops = n // 2
    feats = features // n
    blocked = [one.reshape(blocks, block_len, width) for one in (queries, gate_pre, cotangent)]
    vmem = pl.BlockSpec(memory_space=pltpu.VMEM)
    anywhere = pl.BlockSpec(memory_space=pltpu.HBM)
    half, wide = jnp.bfloat16, jnp.float32
    dma = pltpu.SemaphoreType.DMA

    def per_head(shape, kind):
        return [pltpu.VMEM(shape, kind) for _ in range(heads)]

    return pl.pallas_call(
        functools.partial(whole_kernel, n, tp),
        out_shape=(
            jax.ShapeDtypeStruct((tok_rows, width), wide),
            jax.ShapeDtypeStruct((quarter, features), wide),
            jax.ShapeDtypeStruct((feats, width), wide),
        ),
        in_specs=[anywhere] * 9,
        out_specs=(vmem,) * 3,
        scratch_shapes=[
            pltpu.VMEM((1, features), wide),
            pltpu.VMEM((per_block, blocks), jnp.int32),
            pltpu.VMEM((per_block, blocks), jnp.int32),
            pltpu.VMEM((8, 128), wide),
            pltpu.VMEM((blocks, 128), jnp.int32),
            per_head((total, block_len, HD), half),
            per_head((total, block_len, HD), half),
            pltpu.VMEM((n, blocks, 128), jnp.int32),
            pltpu.VMEM((blocks, block_len, width), half),
            pltpu.VMEM((blocks, block_len, width), half),
            pltpu.VMEM((2, CHUNK, features), half),
            pltpu.VMEM((quarter, features), half),
            pltpu.VMEM((rows_dev, features), half),
            pltpu.VMEM((features, 2 * tp * width), half),
            per_head((passages, PLEN, HD), half),
            per_head((passages, PLEN, HD), half),
            pltpu.VMEM((8, 128), jnp.int32),
            pltpu.SMEM((8, 128), jnp.int32),
            per_head((n + 1, 2, blocks, block_len), wide),
            per_head((n, 2, blocks, block_len), wide),
            per_head((total + 4, 2, block_len), wide),
            per_head((total, block_len, HD), half),
            pltpu.VMEM((total, PLEN, HD), half),
            pltpu.VMEM((total, PLEN, HD), half),
            per_head((rows_dev, HD), half),
            per_head((rows_dev, HD), half),
            pltpu.VMEM((heads, HD, rows_dev), half),
            pltpu.VMEM((quarter, 2 * tp * width), half),
            per_head((blocks, block_len, HD), half),
            per_head((2, hops, blocks, block_len, HD), half),
            pltpu.VMEM((heads, HD, feats), half),
            pltpu.VMEM((2 * hops * heads, HD, feats), half),
            dma((heads + 8,)),
            dma((2,)),
            dma((heads, 2)),
            dma((heads, 2, hops, 4)),
            dma((1,)),
            dma((1,)),
            dma((heads, 2)),
            dma((heads, 2)),
            dma((heads,)),
            dma((heads, 2, hops, 4)),
            dma((1,)),
            dma((2, hops, heads)),
            dma((heads, 2)),
            dma((heads, 2)),
            dma((2,)),
            dma((2, 3)),
            dma((1,)),
        ],
        cost_estimate=pl.CostEstimate(flops=2 * 10**10, bytes_accessed=3 * 10**7, transcendentals=0),
        compiler_params=pltpu.CompilerParams(collective_id=0, has_side_effects=True, vmem_limit_bytes=VMEM_LIMIT),
        name="whole",
    )(*[pltpu.with_memory_space_constraint(one, pltpu.HBM) for one in (*blocked, store, w_key, w_value, store_gain[None], owners.T, slots.T)])


def fits(queries, store, owners):
    n, tp = lax.axis_size("st"), lax.axis_size("tp")
    blocks = owners.shape[0]
    block_len = queries.shape[0] // blocks
    slot_cap = (2 * owners.size + n - 1) // n
    return (
        n % 2 == 0 and n >= 8 and tp == 4 and blocks == 8 and n * blocks <= 128
        and block_len == 128 and queries.shape[1] == 2 * HD
        and store.shape[0] % (tp * CHUNK // 2) == 0 and store.shape[0] % 256 == 0
        and store.shape[0] // PLEN <= 128 and store.shape[1] % (256 * n) == 0
        and 8 * slot_cap * PLEN >= 3 * queries.shape[0]
    )


def local(*arrays):
    if fits(arrays[0], arrays[3], arrays[7]):
        return query_plan(*arrays)
    return passage_plan(*arrays)


def solution(mesh):
    placed = (
        P("st", "tp"),
        P("st", "tp"),
        P("st", "tp"),
        P("st", None),
        P(),
        P(None, "tp"),
        P(None, "tp"),
        P("st", None),
        P("st", None),
    )
    return jax.shard_map(
        local,
        mesh=mesh,
        in_specs=placed,
        out_specs=(P("st", "tp"), P(("st", "tp"), None), P("st", "tp")),
        check_vma=False,
    )
```

```python
import functools

import jax
import jax.numpy as jnp
from jax import lax
from jax.experimental import pallas as pl
from jax.experimental.pallas import tpu as pltpu
from jax.sharding import PartitionSpec as P

HD = 128
PLEN = 64


EPS = 1e-06


def row_scale(store_rows):
    return lax.rsqrt(jnp.mean(store_rows * store_rows, axis=-1, keepdims=True) + EPS)


def contract(left, right):
    return lax.dot_general(
        left, right, (((1,), (1,)), ((), ())), preferred_element_type=jnp.float32
    )


def passage_plan(queries, gate_pre, cotangent, store, store_gain, w_key, w_value, owners, slots):
    st_size = lax.axis_size("st")
    tp_size = lax.axis_size("tp")
    blocks, per_block = owners.shape
    tok_rows, local_width = queries.shape
    head_dim = HD
    local_heads = local_width // head_dim
    block_len = tok_rows // blocks
    passage_len = PLEN
    rows_dev = store.shape[0]
    passages = rows_dev // passage_len
    slot_count = blocks * per_block
    slot_cap = (2 * slot_count + st_size - 1) // st_size
    store_rows = store.astype(jnp.float32)
    row_inverse = row_scale(store_rows)
    normed = (store_rows * row_inverse * store_gain).astype(jnp.bfloat16)
    key_table = jnp.dot(normed, w_key, preferred_element_type=jnp.float32).astype(jnp.bfloat16)
    value_table = jnp.dot(normed, w_value, preferred_element_type=jnp.float32).astype(jnp.bfloat16)
    key_table = key_table.reshape(passages, passage_len, local_width)
    value_table = value_table.reshape(passages, passage_len, local_width)
    owner_flat = owners.reshape(slot_count)
    slot_flat = slots.reshape(slot_count)
    slot_order = jnp.arange(slot_count, dtype=jnp.int32)
    earlier_same = (owner_flat[:, None] == owner_flat[None, :]) & (
        slot_order[None, :] < slot_order[:, None]
    )
    slot_rank = jnp.sum(earlier_same.astype(jnp.int32), axis=1)
    position = owner_flat * slot_cap + slot_rank
    places = jnp.arange(st_size * slot_cap, dtype=jnp.int32)
    slot_hits = position[:, None] == places[None, :]
    requests = jnp.sum(jnp.where(slot_hits, slot_flat[:, None], 0), axis=0)
    requests = requests.reshape(st_size, slot_cap)
    asked_ids = lax.all_to_all(requests, "st", split_axis=0, concat_axis=0, tiled=True)
    asked_flat = asked_ids.reshape(-1)
    shape_out = asked_ids.shape + (passage_len, local_width)
    picked_keys = jnp.take(key_table, asked_flat, axis=0).reshape(shape_out)
    picked_values = jnp.take(value_table, asked_flat, axis=0).reshape(shape_out)
    sent_keys = lax.all_to_all(picked_keys, "st", split_axis=0, concat_axis=0, tiled=True)
    sent_values = lax.all_to_all(picked_values, "st", split_axis=0, concat_axis=0, tiled=True)
    got_keys, got_values, asked_ids = (sent_keys, sent_values, asked_ids)
    span = per_block * passage_len
    mine_keys = jnp.take(
        got_keys.reshape(st_size * slot_cap, passage_len, local_width), position, axis=0
    )
    mine_values = jnp.take(
        got_values.reshape(st_size * slot_cap, passage_len, local_width), position, axis=0
    )
    mine_keys = mine_keys.reshape(blocks, span, local_heads, head_dim)
    mine_values = mine_values.reshape(blocks, span, local_heads, head_dim)
    score_scale = head_dim ** (-0.5)
    query_blocks = queries.reshape(blocks, block_len, local_heads, head_dim)
    gate_open = jax.nn.sigmoid(gate_pre.astype(jnp.float32))
    grad_in = (gate_open * cotangent.astype(jnp.float32)).astype(jnp.bfloat16)
    grad_in = grad_in.reshape(blocks, block_len, local_heads, head_dim)
    scores = (
        jnp.einsum("bqhd,bkhd->bhqk", query_blocks, mine_keys, preferred_element_type=jnp.float32)
        * score_scale
    )
    shifted = scores - jnp.max(scores, axis=-1, keepdims=True)
    weights = jnp.exp(shifted)
    weights = weights / jnp.sum(weights, axis=-1, keepdims=True)
    weights_half = weights.astype(jnp.bfloat16)
    attended = jnp.einsum(
        "bhqk,bkhd->bqhd", weights_half, mine_values, preferred_element_type=jnp.float32
    )
    row_delta = jnp.sum(grad_in.astype(jnp.float32) * attended, axis=-1)
    grad_weights = jnp.einsum(
        "bqhd,bkhd->bhqk", grad_in, mine_values, preferred_element_type=jnp.float32
    )
    grad_scores = weights * (grad_weights - jnp.transpose(row_delta, (0, 2, 1))[..., None])
    grad_half = grad_scores.astype(jnp.bfloat16)
    grad_queries = (
        jnp.einsum("bhqk,bkhd->bqhd", grad_half, mine_keys, preferred_element_type=jnp.float32)
        * score_scale
    )
    grad_queries = grad_queries.reshape(tok_rows, local_width)
    grad_keys = (
        jnp.einsum("bhqk,bqhd->bkhd", grad_half, query_blocks, preferred_element_type=jnp.float32)
        * score_scale
    )
    grad_values = jnp.einsum(
        "bhqk,bqhd->bkhd", weights_half, grad_in, preferred_element_type=jnp.float32
    )
    grad_keys = grad_keys.reshape(slot_count, passage_len, local_width)
    grad_values = grad_values.reshape(slot_count, passage_len, local_width)
    empty_slots = jnp.zeros((st_size * slot_cap, passage_len, local_width), jnp.bfloat16)
    outgoing_keys = empty_slots.at[position].set(grad_keys.astype(jnp.bfloat16))
    outgoing_values = empty_slots.at[position].set(grad_values.astype(jnp.bfloat16))
    back_keys, back_values = (
        lax.all_to_all(outgoing_keys, "st", split_axis=0, concat_axis=0, tiled=True),
        lax.all_to_all(outgoing_values, "st", split_axis=0, concat_axis=0, tiled=True),
    )
    asked_flat = asked_ids.reshape(-1)
    owner_pick = (asked_flat[None, :] == jnp.arange(passages, dtype=jnp.int32)[:, None]).astype(
        jnp.bfloat16
    )
    passage_keys = jnp.dot(
        owner_pick,
        back_keys.reshape(st_size * slot_cap, passage_len * local_width),
        preferred_element_type=jnp.float32,
    )
    passage_values = jnp.dot(
        owner_pick,
        back_values.reshape(st_size * slot_cap, passage_len * local_width),
        preferred_element_type=jnp.float32,
    )
    passage_keys = passage_keys.astype(jnp.bfloat16).reshape(rows_dev, local_width)
    passage_values = passage_values.astype(jnp.bfloat16).reshape(rows_dev, local_width)
    weight_terms = lax.dot_general(
        normed, passage_values, (((0,), (0,)), ((), ())), preferred_element_type=jnp.float32
    )
    grad_w_value = lax.psum_scatter(weight_terms, "st", scatter_dimension=0, tiled=True)
    quarter = rows_dev // tp_size
    whole_key, whole_value = (
        lax.all_gather(w_key, "tp", axis=1, tiled=True),
        lax.all_gather(w_value, "tp", axis=1, tiled=True),
    )
    own_keys, own_values = (
        lax.all_to_all(passage_keys, "tp", split_axis=0, concat_axis=1, tiled=True),
        lax.all_to_all(passage_values, "tp", split_axis=0, concat_axis=1, tiled=True),
    )
    grad_normed = contract(own_keys, whole_key) + contract(own_values, whole_value)
    first_row = lax.axis_index("tp") * quarter
    own_rows = lax.dynamic_slice_in_dim(store_rows, first_row, quarter, 0)
    own_inverse = lax.dynamic_slice_in_dim(row_inverse, first_row, quarter, 0)
    unit_rows = own_rows * own_inverse
    grad_unit = grad_normed * store_gain
    grad_store = own_inverse * (
        grad_unit - unit_rows * jnp.mean(grad_unit * unit_rows, axis=-1, keepdims=True)
    )
    return (grad_queries, grad_store, grad_w_value)

FAR = 1e30
MESH = pl.DeviceIdType.MESH
NT = (((1,), (1,)), ((), ()))
TN = (((0,), (0,)), ((), ()))
CHUNK = 128
VMEM_LIMIT = 45 << 20


def place_of(index, n):
    odd = index % 2
    return (1 - odd) * (index // 2) + odd * (n - 1 - index // 2)


def index_at(place, n):
    place = (place + 2 * n) % n
    back = place // (n // 2)
    return (1 - back) * (2 * place) + back * (2 * (n - 1 - place) + 1)


def dot(left, right, dims=(((1,), (0,)), ((), ()))):
    return lax.dot_general(left, right, dims, preferred_element_type=jnp.float32)


def as_float(flag):
    return jnp.where(flag, jnp.float32(1.0), jnp.float32(0.0))


def rows_of_table(named, first, passages):
    total = named.shape[0]
    held = (named - first).astype(jnp.float32)
    inside = (held >= 0.0) & (held < passages)
    col = jnp.max(jnp.where(inside, held, -1.0), axis=1, keepdims=True)
    spot_col = lax.broadcasted_iota(jnp.int32, (128, 128), 0).astype(jnp.float32)
    spot_row = lax.broadcasted_iota(jnp.int32, (128, 128), 1).astype(jnp.float32)
    wide = jnp.broadcast_to(col, (total, 128))
    if total < 128:
        wide = jnp.concatenate([wide, jnp.full((128 - total, 128), 1000.0, jnp.float32)], axis=0)
    ids_row = wide.T
    key_col = wide * 128.0 + spot_col
    key_row = key_col.T
    rank_col = jnp.sum(as_float(key_row < key_col), axis=1, keepdims=True)
    rank_row = jnp.sum(as_float(key_col < key_row), axis=0, keepdims=True)
    order_row = jnp.sum(as_float(rank_col == spot_row) * spot_col, axis=0, keepdims=True)
    last_row = jnp.sum(as_float(wide <= spot_row), axis=0, keepdims=True) - 1.0
    has_row = jnp.max(as_float(wide == spot_row), axis=0, keepdims=True)
    rows = [ids_row[:1], rank_row, order_row, jnp.maximum(last_row, 0.0), has_row, jnp.zeros((3, 128), jnp.float32)]
    return jnp.concatenate(rows, axis=0).astype(jnp.int32)


IDS, RANK, ORDER, LAST, HAS = range(5)


def whole_kernel(n, tp, q_hbm, gate_hbm, cot_hbm, x_hbm, wk_hbm, wv_hbm, gain_hbm, owners_hbm, slots_hbm,
                 dq_ref, gs_ref, gw_ref,
                 gain_ref, owners_buf, slots_buf, flat, named_ref, q_all, g_all, i_all, gate_buf, cot_buf, x_buf, own_x, normed, whole, kt, vt,
                 tab_buf, tab, stats, got, joined, dq_sorted, tk, tv, pk, pv, pv_flip, own_kv,
                 dq_send, dq_recv, w_send, w_recv,
                 in_sem, x_sem, g_send, g_recv, i_send, i_recv, j_send, j_recv,
                 s_send, s_recv, ws_send, ws_recv, p_send, p_recv, t_send, t_recv, tab_sem):
    me, mine = lax.axis_index("st"), lax.axis_index("tp")
    place = place_of(me, n)
    right, left = index_at(place + 1, n), index_at(place - 1, n)
    hops = n // 2
    heads = len(q_all)
    total, block_len = q_all[0].shape[:2]
    blocks = total // n
    passages = kt[0].shape[0]
    rows_dev, features = normed.shape
    quarter = rows_dev // tp
    width = heads * HD
    feats = features // n
    scale = HD ** (-0.5)
    sibling = mine + 1 - 2 * (mine % 2)
    across = (mine + tp // 2) % tp
    half = blocks // 2

    barrier = pltpu.get_barrier_semaphore()
    for away in range(1, n):
        pl.semaphore_signal(barrier, inc=1, device_id={"st": (me + away) % n}, device_id_type=MESH)
    for away in range(1, tp):
        pl.semaphore_signal(barrier, inc=1, device_id={"tp": (mine + away) % tp}, device_id_type=MESH)

    def columns(owner, value):
        return pl.ds(pl.multiple_of(value * tp * width + owner * width, 128), width)

    loads = []
    for head in range(heads):
        loads.append(pltpu.make_async_copy(q_hbm.at[:, :, pl.ds(head * HD, HD)], q_all[head].at[pl.ds(me * blocks, blocks)], in_sem.at[head]))
    load_gate = pltpu.make_async_copy(gate_hbm, gate_buf, in_sem.at[heads])
    load_cot = pltpu.make_async_copy(cot_hbm, cot_buf, in_sem.at[heads + 1])
    load_w = [pltpu.make_async_copy(ref, whole.at[:, columns(mine, number)], in_sem.at[heads + 2 + number]) for number, ref in enumerate((wk_hbm, wv_hbm))]
    load_small = [pltpu.make_async_copy(src, dst, in_sem.at[heads + 5 + number]) for number, (src, dst) in enumerate(((owners_hbm, owners_buf), (slots_hbm, slots_buf), (gain_hbm, gain_ref)))]
    load_own = pltpu.make_async_copy(x_hbm.at[pl.ds(pl.multiple_of(mine * quarter, 16), quarter)], own_x, in_sem.at[heads + 4])

    def load_x(chunk):
        return pltpu.make_async_copy(x_hbm.at[pl.ds(chunk * CHUNK, CHUNK)], x_buf.at[chunk % 2], x_sem.at[chunk % 2])

    for copy in load_small[:2] + loads + [load_gate, load_cot] + load_w + load_small[2:] + [load_x(0), load_own]:
        copy.start()

    def begin(copy):
        copy.start()

    def remote(src, dst, send_sem, recv_sem, **to):
        return pltpu.make_async_remote_copy(src_ref=src, dst_ref=dst, send_sem=send_sem, recv_sem=recv_sem, device_id=to, device_id_type=MESH)

    def whole_batch(ref, send_sem, recv_sem):
        return remote(ref, ref, send_sem, recv_sem, st=right)

    parts = ((0, 0), (0, 1), (1, 0), (1, 1))

    def gather_piece(head, side, step, part):
        number, which = parts[part]
        ref = (q_all, g_all)[number][head]
        origin = index_at(place - step, n) if side == 0 else index_at(place + step, n)
        at = ref.at[pl.ds(origin * blocks + which * half, half)]
        return remote(at, at, g_send.at[head, number], g_recv.at[head, side, step, part], st=right if side == 0 else left)

    def goes(side, step, part):
        return step < hops - 1 or parts[part][1] == side

    def ids_piece(away):
        return remote(named_ref, i_all.at[me], i_send.at[0], i_recv.at[0], st=(me + away) % n)

    def weight_piece(number, way):
        owner = mine if way < 2 else across
        at = whole.at[:, columns(owner, number)]
        return remote(at, at, t_send.at[number], t_recv.at[number, way], tp=across if way == 1 else sibling)

    def make_grad_in():
        load_gate.wait()
        load_cot.wait()

        @pl.loop(0, blocks)
        def _(block):
            for head in range(heads):
                cols = pl.ds(head * HD, HD)
                opened = jax.nn.sigmoid(gate_buf[block, :, cols].astype(jnp.float32))
                g_all[head][me * blocks + block] = (opened * cot_buf[block, :, cols].astype(jnp.float32)).astype(jnp.bfloat16)

    def project(chunk):
        if (chunk + 1) * CHUNK < rows_dev:
            load_x(chunk + 1).start()
        load_x(chunk).wait()
        rows = pl.ds(chunk * CHUNK, CHUNK)
        wide = x_buf[chunk % 2].astype(jnp.float32)
        ready = (wide * row_scale(wide) * gain_ref[...]).astype(jnp.bfloat16)
        normed[rows] = ready
        per = CHUNK // PLEN
        for number, table in enumerate((kt, vt)):
            out = dot(ready, whole[:, columns(mine, number)]).astype(jnp.bfloat16)
            for head in range(heads):
                table[head][pl.ds(chunk * per, per)] = out[:, head * HD:(head + 1) * HD].reshape(per, PLEN, HD)

    def make_table():
        whole_batch(i_all.at[pl.ds(0, n - 1)], i_send.at[0], i_recv.at[0]).wait_recv()
        tab_buf[...] = rows_of_table(i_all[...].reshape(total, 128), me * passages, passages)
        copy = pltpu.make_async_copy(tab_buf, tab, tab_sem.at[0])
        copy.start()
        copy.wait()

    def make_stats(head, origin):
        for first in range(0, blocks, 4):
            count = min(4, blocks - first)
            spots = [origin * blocks + first + lane for lane in range(count)]
            ids = [jnp.minimum(tab[IDS, spot], passages - 1) for spot in spots]
            scores = [dot(kt[head][jnp.maximum(one, 0)], q_all[head][spot], NT) * scale for one, spot in zip(ids, spots)]
            grads = [dot(vt[head][jnp.maximum(one, 0)], g_all[head][spot], NT) for one, spot in zip(ids, spots)]
            tops = [jnp.max(one, axis=0, keepdims=True) for one in scores]
            raised = [jnp.exp(one - top) for one, top in zip(scores, tops)]
            totals = [jnp.sum(one, axis=0, keepdims=True) for one in raised]
            means = [jnp.sum(one * two, axis=0, keepdims=True) / three for one, two, three in zip(raised, grads, totals)]
            for lane in range(count):
                dead = jnp.minimum(ids[lane], 0).astype(jnp.float32) * FAR
                stats[head][origin, 0, pl.ds(first + lane, 1)] = tops[lane] + jnp.log(totals[lane]) + dead
                stats[head][origin, 1, pl.ds(first + lane, 1)] = means[lane]

    def join_piece(head, phase, away):
        peer = (me + away) % n
        at = joined[head].at[pl.ds(me * blocks, blocks)]
        return remote(
            stats[head].at[peer] if phase == 0 else at,
            got[head].at[me] if phase == 0 else at,
            j_send.at[head, phase], j_recv.at[head, phase], st=peer)

    def join_batch(head, phase):
        ref = got[head].at[pl.ds(0, n - 1)] if phase == 0 else joined[head].at[pl.ds(0, (n - 1) * blocks)]
        return whole_batch(ref, j_send.at[head, phase], j_recv.at[head, phase])

    def join_first(head):
        for away in range(1, n):
            begin(join_piece(head, 0, away))
        got[head][me] = stats[head][me]

    def join_second(head):
        join_batch(head, 0).wait_recv()
        logs = [got[head][owner, 0] for owner in range(n)]
        top = functools.reduce(jnp.maximum, logs)
        shares = [jnp.exp(one - top) for one in logs]
        whole_sum = sum(shares)
        final = top + jnp.log(whole_sum)
        mean = sum(share * got[head][owner, 1] for owner, share in enumerate(shares)) / whole_sum
        for block in range(blocks):
            joined[head][me * blocks + block, 0:1] = final[block:block + 1]
            joined[head][me * blocks + block, 1:2] = mean[block:block + 1]
        for away in range(1, n):
            begin(join_piece(head, 1, away))

    def join_last(head):
        join_batch(head, 1).wait_recv()

    lanes = 4

    def make_grads(head, begin_turn, end_turn, carry):
        def turn_body(turn, carry):
            acc_k, acc_v, past = carry
            spots = [jnp.clip(tab[ORDER, turn * lanes + lane], 0, total - 1) for lane in range(lanes)]
            ids = [jnp.minimum(tab[IDS, spot], passages - 1) for spot in spots]
            keys = [kt[head][jnp.maximum(one, 0)] for one in ids]
            queries = [q_all[head][spot] for spot in spots]
            givens = [g_all[head][spot] for spot in spots]
            scores = [dot(key, query, NT) * scale for key, query in zip(keys, queries)]
            grads = [dot(vt[head][jnp.maximum(one, 0)], given, NT) for one, given in zip(ids, givens)]
            weights, halves = [], []
            for one, spot, score, grad in zip(ids, spots, scores, grads):
                logs = joined[head][spot, 0:1] - jnp.minimum(one, 0).astype(jnp.float32) * FAR
                weight = jnp.exp(score - logs)
                halves.append((weight * (grad - joined[head][spot, 1:2])).astype(jnp.bfloat16))
                weights.append(weight.astype(jnp.bfloat16))
            term_k = [dot(one, query) for one, query in zip(halves, queries)]
            term_v = [dot(one, given) for one, given in zip(weights, givens)]
            steps = [dot(one, key, TN) for one, key in zip(halves, keys)]
            for lane in range(lanes):
                keep = as_float(ids[lane] == past)
                past = ids[lane]
                acc_k = acc_k * keep + term_k[lane]
                acc_v = acc_v * keep + term_v[lane]
                at = turn * lanes + lane
                tk[at] = (acc_k * scale).astype(jnp.bfloat16)
                tv[at] = acc_v.astype(jnp.bfloat16)
                dq_sorted[head][at] = (steps[lane] * scale).astype(jnp.bfloat16)
            return acc_k, acc_v, past

        return lax.fori_loop(begin_turn, end_turn, turn_body, carry)

    blank = (jnp.zeros((PLEN, HD), jnp.float32), jnp.zeros((PLEN, HD), jnp.float32), jnp.int32(-2))
    turns = total // lanes

    def pick(head):
        @pl.loop(0, passages)
        def _(passage):
            last = jnp.clip(tab[LAST, passage], 0, total - 1)
            has = tab[HAS, passage].astype(jnp.float32)
            rows = pl.ds(pl.multiple_of(passage * PLEN, PLEN), PLEN)
            pk[head][rows] = (tk[last].astype(jnp.float32) * has).astype(jnp.bfloat16)
            pv[head][rows] = (tv[last].astype(jnp.float32) * has).astype(jnp.bfloat16)

    def own_columns(owner, head, number):
        return pl.ds(pl.multiple_of(number * tp * width + owner * width + head * HD, 128), HD)

    def passage_piece(head, number, away):
        peer = (mine + away) % tp
        rows = pl.ds(pl.multiple_of(peer * quarter, 16), quarter)
        return remote((pk, pv)[number][head].at[rows], own_kv.at[:, own_columns(mine, head, number)],
                      p_send.at[head, number], p_recv.at[head, number], tp=peer)

    def passage_batch(head, number):
        ref = (pk, pv)[number][head].at[pl.ds(0, (tp - 1) * quarter)]
        return remote(ref, ref, p_send.at[head, number], p_recv.at[head, number], tp=sibling)

    def share(head):
        for number in range(2):
            for away in range(1, tp):
                begin(passage_piece(head, number, away))
            rows = pl.ds(pl.multiple_of(mine * quarter, 16), quarter)
            own_kv[:, own_columns(mine, head, number)] = (pk, pv)[number][head][rows]

    dq_parts = ((0, 0), (half, 1), (half // 2, 0), (half + half // 2, 1))
    dq_count = half // 2

    def used(side, step, part):
        return step > 0 or dq_parts[part][1] == side

    def dq_piece(head, side, step, part):
        at = pl.ds(dq_parts[part][0], dq_count)
        src = dq_recv[head].at[side, step - 1, at] if step > 0 else dq_send[head].at[at]
        return remote(src, dq_recv[head].at[side, step, at],
                      s_send.at[head], s_recv.at[head, side, step, part], st=right if side == 0 else left)

    def dest_of(side, step):
        distance = hops - step
        return index_at(place + distance, n) if side == 0 else index_at(place - distance, n)

    def dq_step(head, step, part):
        for side in range(2):
            if not used(side, step, part):
                continue
            dest = dest_of(side, step)
            arrived = step > 0 and used(side, step - 1, part)
            if arrived:
                dq_piece(head, side, step - 1, part).wait_recv()
            for lane in range(dq_count):
                block = dq_parts[part][0] + lane
                value = dq_sorted[head][jnp.clip(tab[RANK, dest * blocks + block], 0, total - 1)]
                if arrived:
                    value = (value.astype(jnp.float32) + dq_recv[head][side, step - 1, block].astype(jnp.float32)).astype(jnp.bfloat16)
                if step > 0:
                    dq_recv[head][side, step - 1, block] = value
                else:
                    dq_send[head][block] = value
            begin(dq_piece(head, side, step, part))

    def dq_end(head, part):
        for side in range(2):
            dq_piece(head, side, hops - 1, part).wait_recv()
        for lane in range(dq_count):
            block = dq_parts[part][0] + lane
            value = dq_sorted[head][jnp.clip(tab[RANK, me * blocks + block], 0, total - 1)].astype(jnp.float32)
            for side in range(2):
                value = value + dq_recv[head][side, hops - 1, block].astype(jnp.float32)
            dq_ref[pl.ds(block * block_len, block_len), pl.ds(head * HD, HD)] = value

    def w_at(side, step, part):
        return (side * hops + step) * heads + part

    def w_piece(side, step, part):
        src = w_recv.at[w_at(side, step - 1, part)] if step > 0 else w_send.at[part]
        return remote(src, w_recv.at[w_at(side, step, part)],
                      ws_send.at[0], ws_recv.at[side, step, part], st=right if side == 0 else left)

    def w_term(dest, part):
        return dot(pv_flip[part], normed[:, pl.ds(pl.multiple_of(dest * feats, 128), feats)])

    def w_used(side, step, part):
        return step > 0 or part % 2 == side

    def w_step(step, part):
        for side in range(2):
            if not w_used(side, step, part):
                continue
            value = w_term(dest_of(side, step), part)
            if step > 0 and w_used(side, step - 1, part):
                w_piece(side, step - 1, part).wait_recv()
                value = value + w_recv[w_at(side, step - 1, part)].astype(jnp.float32)
            if step > 0:
                w_recv[w_at(side, step - 1, part)] = value.astype(jnp.bfloat16)
            else:
                w_send[part] = value.astype(jnp.bfloat16)
            begin(w_piece(side, step, part))

    def w_end(part):
        value = w_term(me, part)
        for side in range(2):
            w_piece(side, hops - 1, part).wait_recv()
            value = value + w_recv[w_at(side, hops - 1, part)].astype(jnp.float32)
        gw_ref[:, pl.ds(part * HD, HD)] = value.T

    def flip(head):
        for first in range(0, rows_dev, 256):
            pv_flip[head, :, pl.ds(first, 256)] = pv[head][pl.ds(first, 256)].astype(jnp.float32).T.astype(jnp.bfloat16)

    slab = 256

    def store_slab(number):
        cols = pl.ds(number * slab, slab)
        gs_ref[:, cols] = dot(own_kv[...], whole[cols], NT) * gain_ref[:, cols]

    def store_end(first, count):
        rows = pl.ds(first, count)
        wide = own_x[rows].astype(jnp.float32)
        inverse = row_scale(wide)
        unit = wide * inverse
        value = gs_ref[rows]
        gs_ref[rows] = inverse * (value - unit * jnp.mean(value * unit, axis=-1, keepdims=True))

    loads[0].wait()
    pl.semaphore_wait(barrier, n - 1 + tp - 1)
    for part in range(2):
        for side in range(2):
            begin(gather_piece(0, side, 0, part))
    make_grad_in()
    for part in range(2, 4):
        for side in range(2):
            begin(gather_piece(0, side, 0, part))
    for copy in load_small[:2]:
        copy.wait()
    per_block = owners_buf.shape[0]
    flat[...] = jnp.full(flat.shape, -1.0, jnp.float32)
    flat[pl.ds(0, per_block), pl.ds(0, blocks)] = (owners_buf[...] * passages + slots_buf[...]).astype(jnp.float32)
    named_ref[...] = jnp.full(named_ref.shape, -1, jnp.int32)
    named_ref[:, pl.ds(0, 8)] = flat[...].T[:blocks].astype(jnp.int32)
    for away in range(1, n):
        begin(ids_piece(away))
    i_all[me] = named_ref[...]
    for copy in load_w:
        copy.wait()
    for number in range(2):
        begin(weight_piece(number, 1))
        begin(weight_piece(number, 0))
    load_small[2].wait()
    for copy in loads[1:]:
        copy.wait()

    tasks = [functools.partial(project, chunk) for chunk in range(rows_dev // CHUNK)]
    tasks.append(make_table)
    tasks.append(functools.partial(make_stats, 0, me))

    def idle():
        pass

    def fill(count=1):
        for _ in range(count):
            if tasks:
                tasks.pop(0)()

    def both(head, step):
        def run():
            make_stats(head, index_at(place - step, n))
            make_stats(head, index_at(place + step, n))
        return run

    state = {0: blank, 1: blank}

    def grads_task(head, first, last):
        def run():
            state[head] = make_grads(head, first, last, state[head])
        return run

    def grad_tasks(head, pieces):
        edges = [turns * piece // pieces for piece in range(pieces + 1)]
        return [grads_task(head, edges[piece], edges[piece + 1]) for piece in range(pieces)]

    def gather_step(head, step):
        for part in range(4):
            for side in range(2):
                if goes(side, step, part):
                    if step > 0:
                        gather_piece(head, side, step - 1, part).wait_recv()
                    begin(gather_piece(head, side, step, part))
            fill()

    def gather_rest(head, first):
        if first:
            for part in range(4):
                for side in range(2):
                    if not goes(side, hops - 1, part):
                        gather_piece(head, side, hops - 2, part).wait_recv()
        else:
            for part in range(4):
                gather_piece(head, parts[part][1], hops - 1, part).wait_recv()

    def forward_weights():
        for number in range(2):
            weight_piece(number, 1).wait_recv()
            begin(weight_piece(number, 2))

    for step in range(1, hops):
        gather_step(0, step)
        if step < hops - 1:
            tasks.append(both(0, step))
    for part in range(4):
        for side in range(2):
            begin(gather_piece(1, side, 0, part))
        fill()
    gather_rest(0, True)
    tasks.append(both(0, hops - 1))
    fill(len(tasks))
    gather_rest(0, False)
    make_stats(0, index_at(place + hops, n))
    join_first(0)
    tasks.extend([functools.partial(make_stats, 1, me), idle, functools.partial(join_second, 0), forward_weights])
    gather_step(1, 1)
    tasks.extend([both(1, 1), idle, idle, functools.partial(join_last, 0)])
    gather_step(1, 2)
    tasks.extend(grad_tasks(0, 4))
    tasks.extend([functools.partial(pick, 0), functools.partial(share, 0), functools.partial(flip, 0)])
    for step in range(3, hops):
        gather_step(1, step)
    fill(len(tasks))
    for part in range(4):
        dq_step(0, 0, part)
    for step in range(2, hops - 1):
        both(1, step)()
    gather_rest(1, True)
    both(1, hops - 1)()
    gather_rest(1, False)
    make_stats(1, index_at(place + hops, n))
    join_first(1)
    for part in range(2):
        dq_step(0, 1, part)
    join_second(1)
    for part in range(2, 4):
        dq_step(0, 1, part)
    w_step(0, 0)
    for part in range(2):
        dq_step(0, 2, part)
    join_last(1)
    tasks.extend(grad_tasks(1, 8))
    for part in range(2, 4):
        dq_step(0, 2, part)
        fill()
    w_step(1, 0)
    fill()
    for step in range(3, hops):
        for part in range(4):
            dq_step(0, step, part)
            fill()
    fill(len(tasks))
    for part in range(4):
        dq_step(1, 0, part)
    w_step(2, 0)
    pick(1)
    share(1)
    flip(1)
    w_step(0, 1)
    for part in range(4):
        dq_end(0, part)
    for part in range(4):
        dq_step(1, 1, part)
    w_step(3, 0)
    w_step(1, 1)
    for number in range(2):
        for way in (0, 2):
            weight_piece(number, way).wait_recv()
    for head in range(heads):
        for number in range(2):
            passage_batch(head, number).wait_recv()
    load_own.wait()
    tasks.extend([functools.partial(store_slab, number) for number in range(features // slab)])
    ending = 64
    tasks.extend([functools.partial(store_end, first, min(ending, quarter - first)) for first in range(0, quarter, ending)])
    tasks.append(functools.partial(w_end, 0))
    for step in range(2, hops):
        for part in range(4):
            dq_step(1, step, part)
            fill()
        w_step(step, 1)
        fill()
    fill(len(tasks))
    for part in range(4):
        dq_end(1, part)
    w_end(1)
    for head in range(heads):
        for number in range(2):
            ref = (q_all, g_all)[number][head].at[pl.ds(0, (n - 1) * blocks)]
            whole_batch(ref, g_send.at[head, number], g_recv.at[head, 0, 0, 0]).wait_send()
            join_batch(head, number).wait_send()
            passage_batch(head, number).wait_send()
        whole_batch(dq_sorted[head].at[pl.ds(0, (n - 1) * blocks)], s_send.at[head], s_recv.at[head, 0, 0, 0]).wait_send()
    for number in range(2):
        ref = whole.at[:, pl.ds(0, (tp - 1) * width)]
        remote(ref, ref, t_send.at[number], t_recv.at[number, 0], tp=sibling).wait_send()
    whole_batch(w_recv.at[pl.ds(0, (n - 1) * heads)], ws_send.at[0], ws_recv.at[0, 0, 0]).wait_send()
    whole_batch(i_all.at[pl.ds(0, n - 1)], i_send.at[0], i_recv.at[0]).wait_send()


def put_kernel(dq_ref, gs_ref, gw_ref, dq_out, gs_out, gw_out, sem):
    copies = [
        pltpu.make_async_copy(src, dst, sem.at[number])
        for number, (src, dst) in enumerate(((gs_ref, gs_out), (dq_ref, dq_out), (gw_ref, gw_out)))
    ]
    for copy in copies:
        copy.start()
    for copy in copies:
        copy.wait()


def query_plan(queries, gate_pre, cotangent, store, store_gain, w_key, w_value, owners, slots):
    n = lax.axis_size("st")
    tp = lax.axis_size("tp")
    blocks, per_block = owners.shape
    tok_rows, width = queries.shape
    heads = width // HD
    block_len = tok_rows // blocks
    rows_dev, features = store.shape
    passages = rows_dev // PLEN
    quarter = rows_dev // tp
    total = n * blocks
    hops = n // 2
    feats = features // n
    blocked = [one.reshape(blocks, block_len, width) for one in (queries, gate_pre, cotangent)]
    vmem = pl.BlockSpec(memory_space=pltpu.VMEM)
    anywhere = pl.BlockSpec(memory_space=pltpu.HBM)
    half, wide = jnp.bfloat16, jnp.float32
    dma = pltpu.SemaphoreType.DMA

    def per_head(shape, kind):
        return [pltpu.VMEM(shape, kind) for _ in range(heads)]

    results = pl.pallas_call(
        functools.partial(whole_kernel, n, tp),
        out_shape=(
            jax.ShapeDtypeStruct((tok_rows, width), wide),
            jax.ShapeDtypeStruct((quarter, features), wide),
            jax.ShapeDtypeStruct((feats, width), wide),
        ),
        in_specs=[anywhere] * 9,
        out_specs=(vmem,) * 3,
        scratch_shapes=[
            pltpu.VMEM((1, features), wide),
            pltpu.VMEM((per_block, blocks), jnp.int32),
            pltpu.VMEM((per_block, blocks), jnp.int32),
            pltpu.VMEM((8, 128), wide),
            pltpu.VMEM((blocks, 128), jnp.int32),
            per_head((total, block_len, HD), half),
            per_head((total, block_len, HD), half),
            pltpu.VMEM((n, blocks, 128), jnp.int32),
            pltpu.VMEM((blocks, block_len, width), half),
            pltpu.VMEM((blocks, block_len, width), half),
            pltpu.VMEM((2, CHUNK, features), half),
            pltpu.VMEM((quarter, features), half),
            pltpu.VMEM((rows_dev, features), half),
            pltpu.VMEM((features, 2 * tp * width), half),
            per_head((passages, PLEN, HD), half),
            per_head((passages, PLEN, HD), half),
            pltpu.VMEM((8, 128), jnp.int32),
            pltpu.SMEM((8, 128), jnp.int32),
            per_head((n + 1, 2, blocks, block_len), wide),
            per_head((n, 2, blocks, block_len), wide),
            per_head((total + 4, 2, block_len), wide),
            per_head((total, block_len, HD), half),
            pltpu.VMEM((total, PLEN, HD), half),
            pltpu.VMEM((total, PLEN, HD), half),
            per_head((rows_dev, HD), half),
            per_head((rows_dev, HD), half),
            pltpu.VMEM((heads, HD, rows_dev), half),
            pltpu.VMEM((quarter, 2 * tp * width), half),
            per_head((blocks, block_len, HD), half),
            per_head((2, hops, blocks, block_len, HD), half),
            pltpu.VMEM((heads, HD, feats), half),
            pltpu.VMEM((2 * hops * heads, HD, feats), half),
            dma((heads + 8,)),
            dma((2,)),
            dma((heads, 2)),
            dma((heads, 2, hops, 4)),
            dma((1,)),
            dma((1,)),
            dma((heads, 2)),
            dma((heads, 2)),
            dma((heads,)),
            dma((heads, 2, hops, 4)),
            dma((1,)),
            dma((2, hops, heads)),
            dma((heads, 2)),
            dma((heads, 2)),
            dma((2,)),
            dma((2, 3)),
            dma((1,)),
        ],
        cost_estimate=pl.CostEstimate(flops=2 * 10**10, bytes_accessed=3 * 10**7, transcendentals=0),
        compiler_params=pltpu.CompilerParams(collective_id=0, has_side_effects=True, vmem_limit_bytes=VMEM_LIMIT),
        name="whole",
    )(*[pltpu.with_memory_space_constraint(one, pltpu.HBM) for one in (*blocked, store, w_key, w_value, store_gain[None], owners.T, slots.T)])
    return pl.pallas_call(
        put_kernel,
        out_shape=tuple(jax.ShapeDtypeStruct(one.shape, one.dtype) for one in results),
        in_specs=[vmem] * 3,
        out_specs=(anywhere,) * 3,
        scratch_shapes=[dma((3,))],
        cost_estimate=pl.CostEstimate(flops=10**7, bytes_accessed=8 * 10**6, transcendentals=0),
        compiler_params=pltpu.CompilerParams(vmem_limit_bytes=8 << 20),
        name="put",
    )(*results)


def fits(queries, store, owners):
    n, tp = lax.axis_size("st"), lax.axis_size("tp")
    blocks = owners.shape[0]
    block_len = queries.shape[0] // blocks
    slot_cap = (2 * owners.size + n - 1) // n
    return (
        n % 2 == 0 and n >= 8 and tp == 4 and blocks == 8 and n * blocks <= 128
        and block_len == 128 and queries.shape[1] == 2 * HD
        and store.shape[0] % (tp * CHUNK // 2) == 0 and store.shape[0] % 256 == 0
        and store.shape[0] // PLEN <= 128 and store.shape[1] % (256 * n) == 0
        and 8 * slot_cap * PLEN >= 3 * queries.shape[0]
    )


def local(*arrays):
    if fits(arrays[0], arrays[3], arrays[7]):
        return query_plan(*arrays)
    return passage_plan(*arrays)


def solution(mesh):
    placed = (
        P("st", "tp"),
        P("st", "tp"),
        P("st", "tp"),
        P("st", None),
        P(),
        P(None, "tp"),
        P(None, "tp"),
        P("st", None),
        P("st", None),
    )
    return jax.shard_map(
        local,
        mesh=mesh,
        in_specs=placed,
        out_specs=(P("st", "tp"), P(("st", "tp"), None), P("st", "tp")),
        check_vma=False,
    )
```

```python
import functools

import jax
import jax.numpy as jnp
from jax import lax
from jax.experimental import pallas as pl
from jax.experimental.pallas import tpu as pltpu
from jax.sharding import PartitionSpec as P

HD = 128
PLEN = 64


EPS = 1e-06


def row_scale(store_rows):
    return lax.rsqrt(jnp.mean(store_rows * store_rows, axis=-1, keepdims=True) + EPS)


def contract(left, right):
    return lax.dot_general(
        left, right, (((1,), (1,)), ((), ())), preferred_element_type=jnp.float32
    )


def passage_plan(queries, gate_pre, cotangent, store, store_gain, w_key, w_value, owners, slots):
    st_size = lax.axis_size("st")
    tp_size = lax.axis_size("tp")
    blocks, per_block = owners.shape
    tok_rows, local_width = queries.shape
    head_dim = HD
    local_heads = local_width // head_dim
    block_len = tok_rows // blocks
    passage_len = PLEN
    rows_dev = store.shape[0]
    passages = rows_dev // passage_len
    slot_count = blocks * per_block
    slot_cap = (2 * slot_count + st_size - 1) // st_size
    store_rows = store.astype(jnp.float32)
    row_inverse = row_scale(store_rows)
    normed = (store_rows * row_inverse * store_gain).astype(jnp.bfloat16)
    key_table = jnp.dot(normed, w_key, preferred_element_type=jnp.float32).astype(jnp.bfloat16)
    value_table = jnp.dot(normed, w_value, preferred_element_type=jnp.float32).astype(jnp.bfloat16)
    key_table = key_table.reshape(passages, passage_len, local_width)
    value_table = value_table.reshape(passages, passage_len, local_width)
    owner_flat = owners.reshape(slot_count)
    slot_flat = slots.reshape(slot_count)
    slot_order = jnp.arange(slot_count, dtype=jnp.int32)
    earlier_same = (owner_flat[:, None] == owner_flat[None, :]) & (
        slot_order[None, :] < slot_order[:, None]
    )
    slot_rank = jnp.sum(earlier_same.astype(jnp.int32), axis=1)
    position = owner_flat * slot_cap + slot_rank
    places = jnp.arange(st_size * slot_cap, dtype=jnp.int32)
    slot_hits = position[:, None] == places[None, :]
    requests = jnp.sum(jnp.where(slot_hits, slot_flat[:, None], 0), axis=0)
    requests = requests.reshape(st_size, slot_cap)
    asked_ids = lax.all_to_all(requests, "st", split_axis=0, concat_axis=0, tiled=True)
    asked_flat = asked_ids.reshape(-1)
    shape_out = asked_ids.shape + (passage_len, local_width)
    picked_keys = jnp.take(key_table, asked_flat, axis=0).reshape(shape_out)
    picked_values = jnp.take(value_table, asked_flat, axis=0).reshape(shape_out)
    sent_keys = lax.all_to_all(picked_keys, "st", split_axis=0, concat_axis=0, tiled=True)
    sent_values = lax.all_to_all(picked_values, "st", split_axis=0, concat_axis=0, tiled=True)
    got_keys, got_values, asked_ids = (sent_keys, sent_values, asked_ids)
    span = per_block * passage_len
    mine_keys = jnp.take(
        got_keys.reshape(st_size * slot_cap, passage_len, local_width), position, axis=0
    )
    mine_values = jnp.take(
        got_values.reshape(st_size * slot_cap, passage_len, local_width), position, axis=0
    )
    mine_keys = mine_keys.reshape(blocks, span, local_heads, head_dim)
    mine_values = mine_values.reshape(blocks, span, local_heads, head_dim)
    score_scale = head_dim ** (-0.5)
    query_blocks = queries.reshape(blocks, block_len, local_heads, head_dim)
    gate_open = jax.nn.sigmoid(gate_pre.astype(jnp.float32))
    grad_in = (gate_open * cotangent.astype(jnp.float32)).astype(jnp.bfloat16)
    grad_in = grad_in.reshape(blocks, block_len, local_heads, head_dim)
    scores = (
        jnp.einsum("bqhd,bkhd->bhqk", query_blocks, mine_keys, preferred_element_type=jnp.float32)
        * score_scale
    )
    shifted = scores - jnp.max(scores, axis=-1, keepdims=True)
    weights = jnp.exp(shifted)
    weights = weights / jnp.sum(weights, axis=-1, keepdims=True)
    weights_half = weights.astype(jnp.bfloat16)
    attended = jnp.einsum(
        "bhqk,bkhd->bqhd", weights_half, mine_values, preferred_element_type=jnp.float32
    )
    row_delta = jnp.sum(grad_in.astype(jnp.float32) * attended, axis=-1)
    grad_weights = jnp.einsum(
        "bqhd,bkhd->bhqk", grad_in, mine_values, preferred_element_type=jnp.float32
    )
    grad_scores = weights * (grad_weights - jnp.transpose(row_delta, (0, 2, 1))[..., None])
    grad_half = grad_scores.astype(jnp.bfloat16)
    grad_queries = (
        jnp.einsum("bhqk,bkhd->bqhd", grad_half, mine_keys, preferred_element_type=jnp.float32)
        * score_scale
    )
    grad_queries = grad_queries.reshape(tok_rows, local_width)
    grad_keys = (
        jnp.einsum("bhqk,bqhd->bkhd", grad_half, query_blocks, preferred_element_type=jnp.float32)
        * score_scale
    )
    grad_values = jnp.einsum(
        "bhqk,bqhd->bkhd", weights_half, grad_in, preferred_element_type=jnp.float32
    )
    grad_keys = grad_keys.reshape(slot_count, passage_len, local_width)
    grad_values = grad_values.reshape(slot_count, passage_len, local_width)
    empty_slots = jnp.zeros((st_size * slot_cap, passage_len, local_width), jnp.bfloat16)
    outgoing_keys = empty_slots.at[position].set(grad_keys.astype(jnp.bfloat16))
    outgoing_values = empty_slots.at[position].set(grad_values.astype(jnp.bfloat16))
    back_keys, back_values = (
        lax.all_to_all(outgoing_keys, "st", split_axis=0, concat_axis=0, tiled=True),
        lax.all_to_all(outgoing_values, "st", split_axis=0, concat_axis=0, tiled=True),
    )
    asked_flat = asked_ids.reshape(-1)
    owner_pick = (asked_flat[None, :] == jnp.arange(passages, dtype=jnp.int32)[:, None]).astype(
        jnp.bfloat16
    )
    passage_keys = jnp.dot(
        owner_pick,
        back_keys.reshape(st_size * slot_cap, passage_len * local_width),
        preferred_element_type=jnp.float32,
    )
    passage_values = jnp.dot(
        owner_pick,
        back_values.reshape(st_size * slot_cap, passage_len * local_width),
        preferred_element_type=jnp.float32,
    )
    passage_keys = passage_keys.astype(jnp.bfloat16).reshape(rows_dev, local_width)
    passage_values = passage_values.astype(jnp.bfloat16).reshape(rows_dev, local_width)
    weight_terms = lax.dot_general(
        normed, passage_values, (((0,), (0,)), ((), ())), preferred_element_type=jnp.float32
    )
    grad_w_value = lax.psum_scatter(weight_terms, "st", scatter_dimension=0, tiled=True)
    quarter = rows_dev // tp_size
    whole_key, whole_value = (
        lax.all_gather(w_key, "tp", axis=1, tiled=True),
        lax.all_gather(w_value, "tp", axis=1, tiled=True),
    )
    own_keys, own_values = (
        lax.all_to_all(passage_keys, "tp", split_axis=0, concat_axis=1, tiled=True),
        lax.all_to_all(passage_values, "tp", split_axis=0, concat_axis=1, tiled=True),
    )
    grad_normed = contract(own_keys, whole_key) + contract(own_values, whole_value)
    first_row = lax.axis_index("tp") * quarter
    own_rows = lax.dynamic_slice_in_dim(store_rows, first_row, quarter, 0)
    own_inverse = lax.dynamic_slice_in_dim(row_inverse, first_row, quarter, 0)
    unit_rows = own_rows * own_inverse
    grad_unit = grad_normed * store_gain
    grad_store = own_inverse * (
        grad_unit - unit_rows * jnp.mean(grad_unit * unit_rows, axis=-1, keepdims=True)
    )
    return (grad_queries, grad_store, grad_w_value)

FAR = 1e30
MESH = pl.DeviceIdType.MESH
NT = (((1,), (1,)), ((), ()))
TN = (((0,), (0,)), ((), ()))
CHUNK = 128
VMEM_LIMIT = 45 << 20


def place_of(index, n):
    odd = index % 2
    return (1 - odd) * (index // 2) + odd * (n - 1 - index // 2)


def index_at(place, n):
    place = (place + 2 * n) % n
    back = place // (n // 2)
    return (1 - back) * (2 * place) + back * (2 * (n - 1 - place) + 1)


def dot(left, right, dims=(((1,), (0,)), ((), ()))):
    return lax.dot_general(left, right, dims, preferred_element_type=jnp.float32)


def as_float(flag):
    return jnp.where(flag, jnp.float32(1.0), jnp.float32(0.0))


def rows_of_table(named, first, passages):
    total = named.shape[0]
    held = (named - first).astype(jnp.float32)
    inside = (held >= 0.0) & (held < passages)
    col = jnp.max(jnp.where(inside, held, -1.0), axis=1, keepdims=True)
    spot_col = lax.broadcasted_iota(jnp.int32, (128, 128), 0).astype(jnp.float32)
    spot_row = lax.broadcasted_iota(jnp.int32, (128, 128), 1).astype(jnp.float32)
    wide = jnp.broadcast_to(col, (total, 128))
    if total < 128:
        wide = jnp.concatenate([wide, jnp.full((128 - total, 128), 1000.0, jnp.float32)], axis=0)
    ids_row = wide.T
    key_col = wide * 128.0 + spot_col
    key_row = key_col.T
    rank_col = jnp.sum(as_float(key_row < key_col), axis=1, keepdims=True)
    rank_row = jnp.sum(as_float(key_col < key_row), axis=0, keepdims=True)
    order_row = jnp.sum(as_float(rank_col == spot_row) * spot_col, axis=0, keepdims=True)
    last_row = jnp.sum(as_float(wide <= spot_row), axis=0, keepdims=True) - 1.0
    has_row = jnp.max(as_float(wide == spot_row), axis=0, keepdims=True)
    rows = [ids_row[:1], rank_row, order_row, jnp.maximum(last_row, 0.0), has_row, jnp.zeros((3, 128), jnp.float32)]
    return jnp.concatenate(rows, axis=0).astype(jnp.int32)


IDS, RANK, ORDER, LAST, HAS = range(5)


def whole_kernel(n, tp, q_hbm, gate_hbm, cot_hbm, x_hbm, wk_hbm, wv_hbm, gain_hbm, owners_hbm, slots_hbm,
                 dq_ref, gs_ref, gw_ref,
                 gain_ref, owners_buf, slots_buf, flat, named_ref, q_all, g_all, i_all, gate_buf, cot_buf, x_buf, own_x, normed, whole, kt, vt,
                 tab_buf, tab, stats, got, joined, dq_sorted, tk, tv, pk, pv, pv_flip, own_kv,
                 dq_send, dq_recv, w_send, w_recv,
                 in_sem, x_sem, g_send, g_recv, i_send, i_recv, j_send, j_recv,
                 s_send, s_recv, ws_send, ws_recv, p_send, p_recv, t_send, t_recv, tab_sem):
    me, mine = lax.axis_index("st"), lax.axis_index("tp")
    place = place_of(me, n)
    right, left = index_at(place + 1, n), index_at(place - 1, n)
    hops = n // 2
    heads = len(q_all)
    total, block_len = q_all[0].shape[:2]
    blocks = total // n
    passages = kt[0].shape[0]
    rows_dev, features = normed.shape
    quarter = rows_dev // tp
    width = heads * HD
    feats = features // n
    scale = HD ** (-0.5)
    sibling = mine + 1 - 2 * (mine % 2)
    across = (mine + tp // 2) % tp
    half = blocks // 2

    barrier = pltpu.get_barrier_semaphore()
    for away in range(1, n):
        pl.semaphore_signal(barrier, inc=1, device_id={"st": (me + away) % n}, device_id_type=MESH)
    for away in range(1, tp):
        pl.semaphore_signal(barrier, inc=1, device_id={"tp": (mine + away) % tp}, device_id_type=MESH)

    def columns(owner, value):
        return pl.ds(pl.multiple_of(value * tp * width + owner * width, 128), width)

    loads = []
    for head in range(heads):
        loads.append(pltpu.make_async_copy(q_hbm.at[:, :, pl.ds(head * HD, HD)], q_all[head].at[pl.ds(me * blocks, blocks)], in_sem.at[head]))
    load_gate = pltpu.make_async_copy(gate_hbm, gate_buf, in_sem.at[heads])
    load_cot = pltpu.make_async_copy(cot_hbm, cot_buf, in_sem.at[heads + 1])
    load_w = [pltpu.make_async_copy(ref, whole.at[:, columns(mine, number)], in_sem.at[heads + 2 + number]) for number, ref in enumerate((wk_hbm, wv_hbm))]
    load_small = [pltpu.make_async_copy(src, dst, in_sem.at[heads + 5 + number]) for number, (src, dst) in enumerate(((owners_hbm, owners_buf), (slots_hbm, slots_buf), (gain_hbm, gain_ref)))]
    load_own = pltpu.make_async_copy(x_hbm.at[pl.ds(pl.multiple_of(mine * quarter, 16), quarter)], own_x, in_sem.at[heads + 4])

    def load_x(chunk):
        return pltpu.make_async_copy(x_hbm.at[pl.ds(chunk * CHUNK, CHUNK)], x_buf.at[chunk % 2], x_sem.at[chunk % 2])

    for copy in load_small[:2] + loads + [load_gate, load_cot] + load_w + load_small[2:] + [load_x(0), load_own]:
        copy.start()

    def begin(copy):
        copy.start()

    def remote(src, dst, send_sem, recv_sem, **to):
        return pltpu.make_async_remote_copy(src_ref=src, dst_ref=dst, send_sem=send_sem, recv_sem=recv_sem, device_id=to, device_id_type=MESH)

    def whole_batch(ref, send_sem, recv_sem):
        return remote(ref, ref, send_sem, recv_sem, st=right)

    parts = ((0, 0), (0, 1), (1, 0), (1, 1))

    def gather_piece(head, side, step, part):
        number, which = parts[part]
        ref = (q_all, g_all)[number][head]
        origin = index_at(place - step, n) if side == 0 else index_at(place + step, n)
        at = ref.at[pl.ds(origin * blocks + which * half, half)]
        return remote(at, at, g_send.at[head, number], g_recv.at[head, side, step, part], st=right if side == 0 else left)

    def goes(side, step, part):
        return step < hops - 1 or parts[part][1] == side

    def ids_piece(away):
        return remote(named_ref, i_all.at[me], i_send.at[0], i_recv.at[0], st=(me + away) % n)

    def weight_piece(number, way):
        owner = mine if way < 2 else across
        at = whole.at[:, columns(owner, number)]
        return remote(at, at, t_send.at[number], t_recv.at[number, way], tp=across if way == 1 else sibling)

    def make_grad_in():
        load_gate.wait()
        load_cot.wait()

        @pl.loop(0, blocks)
        def _(block):
            for head in range(heads):
                cols = pl.ds(head * HD, HD)
                opened = jax.nn.sigmoid(gate_buf[block, :, cols].astype(jnp.float32))
                g_all[head][me * blocks + block] = (opened * cot_buf[block, :, cols].astype(jnp.float32)).astype(jnp.bfloat16)

    def project(chunk):
        if (chunk + 1) * CHUNK < rows_dev:
            load_x(chunk + 1).start()
        load_x(chunk).wait()
        rows = pl.ds(chunk * CHUNK, CHUNK)
        wide = x_buf[chunk % 2].astype(jnp.float32)
        ready = (wide * row_scale(wide) * gain_ref[...]).astype(jnp.bfloat16)
        normed[rows] = ready
        per = CHUNK // PLEN
        for number, table in enumerate((kt, vt)):
            out = dot(ready, whole[:, columns(mine, number)]).astype(jnp.bfloat16)
            for head in range(heads):
                table[head][pl.ds(chunk * per, per)] = out[:, head * HD:(head + 1) * HD].reshape(per, PLEN, HD)

    def make_table():
        whole_batch(i_all.at[pl.ds(0, n - 1)], i_send.at[0], i_recv.at[0]).wait_recv()
        tab_buf[...] = rows_of_table(i_all[...].reshape(total, 128), me * passages, passages)
        copy = pltpu.make_async_copy(tab_buf, tab, tab_sem.at[0])
        copy.start()
        copy.wait()

    def make_stats(head, origin):
        for first in range(0, blocks, 4):
            count = min(4, blocks - first)
            spots = [origin * blocks + first + lane for lane in range(count)]
            ids = [jnp.minimum(tab[IDS, spot], passages - 1) for spot in spots]
            scores = [dot(kt[head][jnp.maximum(one, 0)], q_all[head][spot], NT) * scale for one, spot in zip(ids, spots)]
            grads = [dot(vt[head][jnp.maximum(one, 0)], g_all[head][spot], NT) for one, spot in zip(ids, spots)]
            tops = [jnp.max(one, axis=0, keepdims=True) for one in scores]
            raised = [jnp.exp(one - top) for one, top in zip(scores, tops)]
            totals = [jnp.sum(one, axis=0, keepdims=True) for one in raised]
            means = [jnp.sum(one * two, axis=0, keepdims=True) / three for one, two, three in zip(raised, grads, totals)]
            for lane in range(count):
                dead = jnp.minimum(ids[lane], 0).astype(jnp.float32) * FAR
                stats[head][origin, 0, pl.ds(first + lane, 1)] = tops[lane] + jnp.log(totals[lane]) + dead
                stats[head][origin, 1, pl.ds(first + lane, 1)] = means[lane]

    def join_piece(head, phase, away):
        peer = (me + away) % n
        at = joined[head].at[pl.ds(me * blocks, blocks)]
        return remote(
            stats[head].at[peer] if phase == 0 else at,
            got[head].at[me] if phase == 0 else at,
            j_send.at[head, phase], j_recv.at[head, phase], st=peer)

    def join_batch(head, phase):
        ref = got[head].at[pl.ds(0, n - 1)] if phase == 0 else joined[head].at[pl.ds(0, (n - 1) * blocks)]
        return whole_batch(ref, j_send.at[head, phase], j_recv.at[head, phase])

    def join_first(head):
        for away in range(1, n):
            begin(join_piece(head, 0, away))
        got[head][me] = stats[head][me]

    def join_second(head):
        join_batch(head, 0).wait_recv()
        logs = [got[head][owner, 0] for owner in range(n)]
        top = functools.reduce(jnp.maximum, logs)
        shares = [jnp.exp(one - top) for one in logs]
        whole_sum = sum(shares)
        final = top + jnp.log(whole_sum)
        mean = sum(share * got[head][owner, 1] for owner, share in enumerate(shares)) / whole_sum
        for block in range(blocks):
            joined[head][me * blocks + block, 0:1] = final[block:block + 1]
            joined[head][me * blocks + block, 1:2] = mean[block:block + 1]
        for away in range(1, n):
            begin(join_piece(head, 1, away))

    def join_last(head):
        join_batch(head, 1).wait_recv()

    lanes = 4

    def make_grads(head, begin_turn, end_turn, carry):
        def turn_body(turn, carry):
            acc_k, acc_v, past = carry
            spots = [jnp.clip(tab[ORDER, turn * lanes + lane], 0, total - 1) for lane in range(lanes)]
            ids = [jnp.minimum(tab[IDS, spot], passages - 1) for spot in spots]
            keys = [kt[head][jnp.maximum(one, 0)] for one in ids]
            queries = [q_all[head][spot] for spot in spots]
            givens = [g_all[head][spot] for spot in spots]
            scores = [dot(key, query, NT) * scale for key, query in zip(keys, queries)]
            grads = [dot(vt[head][jnp.maximum(one, 0)], given, NT) for one, given in zip(ids, givens)]
            weights, halves = [], []
            for one, spot, score, grad in zip(ids, spots, scores, grads):
                logs = joined[head][spot, 0:1] - jnp.minimum(one, 0).astype(jnp.float32) * FAR
                weight = jnp.exp(score - logs)
                halves.append((weight * (grad - joined[head][spot, 1:2])).astype(jnp.bfloat16))
                weights.append(weight.astype(jnp.bfloat16))
            term_k = [dot(one, query) for one, query in zip(halves, queries)]
            term_v = [dot(one, given) for one, given in zip(weights, givens)]
            steps = [dot(one, key, TN) for one, key in zip(halves, keys)]
            for lane in range(lanes):
                keep = as_float(ids[lane] == past)
                past = ids[lane]
                acc_k = acc_k * keep + term_k[lane]
                acc_v = acc_v * keep + term_v[lane]
                at = turn * lanes + lane
                tk[at] = (acc_k * scale).astype(jnp.bfloat16)
                tv[at] = acc_v.astype(jnp.bfloat16)
                dq_sorted[head][at] = (steps[lane] * scale).astype(jnp.bfloat16)
            return acc_k, acc_v, past

        return lax.fori_loop(begin_turn, end_turn, turn_body, carry)

    blank = (jnp.zeros((PLEN, HD), jnp.float32), jnp.zeros((PLEN, HD), jnp.float32), jnp.int32(-2))
    turns = total // lanes

    def pick(head):
        @pl.loop(0, passages)
        def _(passage):
            last = jnp.clip(tab[LAST, passage], 0, total - 1)
            has = tab[HAS, passage].astype(jnp.float32)
            rows = pl.ds(pl.multiple_of(passage * PLEN, PLEN), PLEN)
            pk[head][rows] = (tk[last].astype(jnp.float32) * has).astype(jnp.bfloat16)
            pv[head][rows] = (tv[last].astype(jnp.float32) * has).astype(jnp.bfloat16)

    def own_columns(owner, head, number):
        return pl.ds(pl.multiple_of(number * tp * width + owner * width + head * HD, 128), HD)

    def passage_piece(head, number, away):
        peer = (mine + away) % tp
        rows = pl.ds(pl.multiple_of(peer * quarter, 16), quarter)
        return remote((pk, pv)[number][head].at[rows], own_kv.at[:, own_columns(mine, head, number)],
                      p_send.at[head, number], p_recv.at[head, number], tp=peer)

    def passage_batch(head, number):
        ref = (pk, pv)[number][head].at[pl.ds(0, (tp - 1) * quarter)]
        return remote(ref, ref, p_send.at[head, number], p_recv.at[head, number], tp=sibling)

    def share(head):
        for number in range(2):
            for away in range(1, tp):
                begin(passage_piece(head, number, away))
            rows = pl.ds(pl.multiple_of(mine * quarter, 16), quarter)
            own_kv[:, own_columns(mine, head, number)] = (pk, pv)[number][head][rows]

    dq_parts = ((0, 0), (half, 1), (half // 2, 0), (half + half // 2, 1))
    dq_count = half // 2

    def used(side, step, part):
        return step > 0 or dq_parts[part][1] == side

    def dq_piece(head, side, step, part):
        at = pl.ds(dq_parts[part][0], dq_count)
        src = dq_recv[head].at[side, step - 1, at] if step > 0 else dq_send[head].at[at]
        return remote(src, dq_recv[head].at[side, step, at],
                      s_send.at[head], s_recv.at[head, side, step, part], st=right if side == 0 else left)

    def dest_of(side, step):
        distance = hops - step
        return index_at(place + distance, n) if side == 0 else index_at(place - distance, n)

    def dq_step(head, step, part):
        for side in range(2):
            if not used(side, step, part):
                continue
            dest = dest_of(side, step)
            arrived = step > 0 and used(side, step - 1, part)
            if arrived:
                dq_piece(head, side, step - 1, part).wait_recv()
            for lane in range(dq_count):
                block = dq_parts[part][0] + lane
                value = dq_sorted[head][jnp.clip(tab[RANK, dest * blocks + block], 0, total - 1)]
                if arrived:
                    value = (value.astype(jnp.float32) + dq_recv[head][side, step - 1, block].astype(jnp.float32)).astype(jnp.bfloat16)
                if step > 0:
                    dq_recv[head][side, step - 1, block] = value
                else:
                    dq_send[head][block] = value
            begin(dq_piece(head, side, step, part))

    def dq_end(head, part):
        for side in range(2):
            dq_piece(head, side, hops - 1, part).wait_recv()
        for lane in range(dq_count):
            block = dq_parts[part][0] + lane
            value = dq_sorted[head][jnp.clip(tab[RANK, me * blocks + block], 0, total - 1)].astype(jnp.float32)
            for side in range(2):
                value = value + dq_recv[head][side, hops - 1, block].astype(jnp.float32)
            dq_ref[pl.ds(block * block_len, block_len), pl.ds(head * HD, HD)] = value

    def w_at(side, step, part):
        return (side * hops + step) * heads + part

    def w_piece(side, step, part):
        src = w_recv.at[w_at(side, step - 1, part)] if step > 0 else w_send.at[part]
        return remote(src, w_recv.at[w_at(side, step, part)],
                      ws_send.at[0], ws_recv.at[side, step, part], st=right if side == 0 else left)

    def w_term(dest, part):
        return dot(pv_flip[part], normed[:, pl.ds(pl.multiple_of(dest * feats, 128), feats)])

    def w_used(side, step, part):
        return step > 0 or part % 2 == side

    def w_step(step, part):
        for side in range(2):
            if not w_used(side, step, part):
                continue
            value = w_term(dest_of(side, step), part)
            if step > 0 and w_used(side, step - 1, part):
                w_piece(side, step - 1, part).wait_recv()
                value = value + w_recv[w_at(side, step - 1, part)].astype(jnp.float32)
            if step > 0:
                w_recv[w_at(side, step - 1, part)] = value.astype(jnp.bfloat16)
            else:
                w_send[part] = value.astype(jnp.bfloat16)
            begin(w_piece(side, step, part))

    def w_end(part):
        value = w_term(me, part)
        for side in range(2):
            w_piece(side, hops - 1, part).wait_recv()
            value = value + w_recv[w_at(side, hops - 1, part)].astype(jnp.float32)
        gw_ref[:, pl.ds(part * HD, HD)] = value.T

    def flip(head):
        for first in range(0, rows_dev, 256):
            pv_flip[head, :, pl.ds(first, 256)] = pv[head][pl.ds(first, 256)].astype(jnp.float32).T.astype(jnp.bfloat16)

    slab = 256

    def store_slab(number):
        cols = pl.ds(number * slab, slab)
        gs_ref[:, cols] = dot(own_kv[...], whole[cols], NT) * gain_ref[:, cols]

    def store_end(first, count):
        rows = pl.ds(first, count)
        wide = own_x[rows].astype(jnp.float32)
        inverse = row_scale(wide)
        unit = wide * inverse
        value = gs_ref[rows]
        gs_ref[rows] = inverse * (value - unit * jnp.mean(value * unit, axis=-1, keepdims=True))

    loads[0].wait()
    pl.semaphore_wait(barrier, n - 1 + tp - 1)
    for part in range(2):
        for side in range(2):
            begin(gather_piece(0, side, 0, part))
    make_grad_in()
    for part in range(2, 4):
        for side in range(2):
            begin(gather_piece(0, side, 0, part))
    for copy in load_small[:2]:
        copy.wait()
    per_block = owners_buf.shape[0]
    flat[...] = jnp.full(flat.shape, -1.0, jnp.float32)
    flat[pl.ds(0, per_block), pl.ds(0, blocks)] = (owners_buf[...] * passages + slots_buf[...]).astype(jnp.float32)
    named_ref[...] = jnp.full(named_ref.shape, -1, jnp.int32)
    named_ref[:, pl.ds(0, 8)] = flat[...].T[:blocks].astype(jnp.int32)
    for away in range(1, n):
        begin(ids_piece(away))
    i_all[me] = named_ref[...]
    for copy in load_w:
        copy.wait()
    for number in range(2):
        begin(weight_piece(number, 1))
        begin(weight_piece(number, 0))
    load_small[2].wait()
    for copy in loads[1:]:
        copy.wait()

    tasks = [functools.partial(project, chunk) for chunk in range(rows_dev // CHUNK)]
    tasks.append(make_table)
    tasks.append(functools.partial(make_stats, 0, me))

    def idle():
        pass

    def fill(count=1):
        for _ in range(count):
            if tasks:
                tasks.pop(0)()

    def both(head, step):
        def run():
            make_stats(head, index_at(place - step, n))
            make_stats(head, index_at(place + step, n))
        return run

    state = {0: blank, 1: blank}

    def grads_task(head, first, last):
        def run():
            state[head] = make_grads(head, first, last, state[head])
        return run

    def grad_tasks(head, pieces):
        edges = [turns * piece // pieces for piece in range(pieces + 1)]
        return [grads_task(head, edges[piece], edges[piece + 1]) for piece in range(pieces)]

    def gather_step(head, step, count=1):
        for part in range(4):
            for side in range(2):
                if goes(side, step, part):
                    if step > 0:
                        gather_piece(head, side, step - 1, part).wait_recv()
                    begin(gather_piece(head, side, step, part))
            fill(count)

    def gather_rest(head, first):
        if first:
            for part in range(4):
                for side in range(2):
                    if not goes(side, hops - 1, part):
                        gather_piece(head, side, hops - 2, part).wait_recv()
        else:
            for part in range(4):
                gather_piece(head, parts[part][1], hops - 1, part).wait_recv()

    def forward_weights():
        for number in range(2):
            weight_piece(number, 1).wait_recv()
            begin(weight_piece(number, 2))

    for step in range(1, hops):
        gather_step(0, step)
        if step < hops - 1:
            tasks.append(both(0, step))
    for part in range(4):
        for side in range(2):
            begin(gather_piece(1, side, 0, part))
        fill()
    gather_rest(0, True)
    tasks.append(both(0, hops - 1))
    fill(len(tasks))
    gather_rest(0, False)
    make_stats(0, index_at(place + hops, n))
    join_first(0)
    tasks.extend([functools.partial(make_stats, 1, me), idle, functools.partial(join_second, 0), forward_weights])
    gather_step(1, 1)
    tasks.extend([both(1, 1), idle, idle, functools.partial(join_last, 0)])
    gather_step(1, 2)
    tasks.extend(grad_tasks(0, 6))
    for step in range(3, hops):
        gather_step(1, step, 2)
    fill(len(tasks))
    for part in range(4):
        dq_step(0, 0, part)
    pick(0)
    share(0)
    flip(0)
    for step in range(2, hops - 1):
        both(1, step)()
    gather_rest(1, True)
    both(1, hops - 1)()
    gather_rest(1, False)
    make_stats(1, index_at(place + hops, n))
    join_first(1)
    for part in range(2):
        dq_step(0, 1, part)
    join_second(1)
    for part in range(2, 4):
        dq_step(0, 1, part)
    w_step(0, 0)
    for part in range(2):
        dq_step(0, 2, part)
    join_last(1)
    tasks.extend(grad_tasks(1, 8))
    for part in range(2, 4):
        dq_step(0, 2, part)
        fill()
    w_step(1, 0)
    fill()
    for step in range(3, hops):
        for part in range(4):
            dq_step(0, step, part)
            fill()
    fill(len(tasks))
    for part in range(4):
        dq_step(1, 0, part)
    w_step(2, 0)
    pick(1)
    share(1)
    flip(1)
    w_step(0, 1)
    for part in range(4):
        dq_end(0, part)
    for part in range(4):
        dq_step(1, 1, part)
    w_step(3, 0)
    w_step(1, 1)
    for number in range(2):
        for way in (0, 2):
            weight_piece(number, way).wait_recv()
    for head in range(heads):
        for number in range(2):
            passage_batch(head, number).wait_recv()
    load_own.wait()
    tasks.extend([functools.partial(store_slab, number) for number in range(features // slab)])
    ending = 64
    tasks.extend([functools.partial(store_end, first, min(ending, quarter - first)) for first in range(0, quarter, ending)])
    tasks.append(functools.partial(w_end, 0))
    for step in range(2, hops):
        for part in range(4):
            dq_step(1, step, part)
            fill()
        w_step(step, 1)
        fill()
    fill(len(tasks))
    for part in range(4):
        dq_end(1, part)
    w_end(1)
    for head in range(heads):
        for number in range(2):
            ref = (q_all, g_all)[number][head].at[pl.ds(0, (n - 1) * blocks)]
            whole_batch(ref, g_send.at[head, number], g_recv.at[head, 0, 0, 0]).wait_send()
            join_batch(head, number).wait_send()
            passage_batch(head, number).wait_send()
        whole_batch(dq_sorted[head].at[pl.ds(0, (n - 1) * blocks)], s_send.at[head], s_recv.at[head, 0, 0, 0]).wait_send()
    for number in range(2):
        ref = whole.at[:, pl.ds(0, (tp - 1) * width)]
        remote(ref, ref, t_send.at[number], t_recv.at[number, 0], tp=sibling).wait_send()
    whole_batch(w_recv.at[pl.ds(0, (n - 1) * heads)], ws_send.at[0], ws_recv.at[0, 0, 0]).wait_send()
    whole_batch(i_all.at[pl.ds(0, n - 1)], i_send.at[0], i_recv.at[0]).wait_send()


def put_kernel(dq_ref, gs_ref, gw_ref, dq_out, gs_out, gw_out, sem):
    copies = [
        pltpu.make_async_copy(src, dst, sem.at[number])
        for number, (src, dst) in enumerate(((gs_ref, gs_out), (dq_ref, dq_out), (gw_ref, gw_out)))
    ]
    for copy in copies:
        copy.start()
    for copy in copies:
        copy.wait()


def query_plan(queries, gate_pre, cotangent, store, store_gain, w_key, w_value, owners, slots):
    n = lax.axis_size("st")
    tp = lax.axis_size("tp")
    blocks, per_block = owners.shape
    tok_rows, width = queries.shape
    heads = width // HD
    block_len = tok_rows // blocks
    rows_dev, features = store.shape
    passages = rows_dev // PLEN
    quarter = rows_dev // tp
    total = n * blocks
    hops = n // 2
    feats = features // n
    blocked = [one.reshape(blocks, block_len, width) for one in (queries, gate_pre, cotangent)]
    vmem = pl.BlockSpec(memory_space=pltpu.VMEM)
    anywhere = pl.BlockSpec(memory_space=pltpu.HBM)
    half, wide = jnp.bfloat16, jnp.float32
    dma = pltpu.SemaphoreType.DMA

    def per_head(shape, kind):
        return [pltpu.VMEM(shape, kind) for _ in range(heads)]

    results = pl.pallas_call(
        functools.partial(whole_kernel, n, tp),
        out_shape=(
            jax.ShapeDtypeStruct((tok_rows, width), wide),
            jax.ShapeDtypeStruct((quarter, features), wide),
            jax.ShapeDtypeStruct((feats, width), wide),
        ),
        in_specs=[anywhere] * 9,
        out_specs=(vmem,) * 3,
        scratch_shapes=[
            pltpu.VMEM((1, features), wide),
            pltpu.VMEM((per_block, blocks), jnp.int32),
            pltpu.VMEM((per_block, blocks), jnp.int32),
            pltpu.VMEM((8, 128), wide),
            pltpu.VMEM((blocks, 128), jnp.int32),
            per_head((total, block_len, HD), half),
            per_head((total, block_len, HD), half),
            pltpu.VMEM((n, blocks, 128), jnp.int32),
            pltpu.VMEM((blocks, block_len, width), half),
            pltpu.VMEM((blocks, block_len, width), half),
            pltpu.VMEM((2, CHUNK, features), half),
            pltpu.VMEM((quarter, features), half),
            pltpu.VMEM((rows_dev, features), half),
            pltpu.VMEM((features, 2 * tp * width), half),
            per_head((passages, PLEN, HD), half),
            per_head((passages, PLEN, HD), half),
            pltpu.VMEM((8, 128), jnp.int32),
            pltpu.SMEM((8, 128), jnp.int32),
            per_head((n + 1, 2, blocks, block_len), wide),
            per_head((n, 2, blocks, block_len), wide),
            per_head((total + 4, 2, block_len), wide),
            per_head((total, block_len, HD), half),
            pltpu.VMEM((total, PLEN, HD), half),
            pltpu.VMEM((total, PLEN, HD), half),
            per_head((rows_dev, HD), half),
            per_head((rows_dev, HD), half),
            pltpu.VMEM((heads, HD, rows_dev), half),
            pltpu.VMEM((quarter, 2 * tp * width), half),
            per_head((blocks, block_len, HD), half),
            per_head((2, hops, blocks, block_len, HD), half),
            pltpu.VMEM((heads, HD, feats), half),
            pltpu.VMEM((2 * hops * heads, HD, feats), half),
            dma((heads + 8,)),
            dma((2,)),
            dma((heads, 2)),
            dma((heads, 2, hops, 4)),
            dma((1,)),
            dma((1,)),
            dma((heads, 2)),
            dma((heads, 2)),
            dma((heads,)),
            dma((heads, 2, hops, 4)),
            dma((1,)),
            dma((2, hops, heads)),
            dma((heads, 2)),
            dma((heads, 2)),
            dma((2,)),
            dma((2, 3)),
            dma((1,)),
        ],
        cost_estimate=pl.CostEstimate(flops=2 * 10**10, bytes_accessed=3 * 10**7, transcendentals=0),
        compiler_params=pltpu.CompilerParams(collective_id=0, has_side_effects=True, vmem_limit_bytes=VMEM_LIMIT),
        name="whole",
    )(*[pltpu.with_memory_space_constraint(one, pltpu.HBM) for one in (*blocked, store, w_key, w_value, store_gain[None], owners.T, slots.T)])
    return pl.pallas_call(
        put_kernel,
        out_shape=tuple(jax.ShapeDtypeStruct(one.shape, one.dtype) for one in results),
        in_specs=[vmem] * 3,
        out_specs=(anywhere,) * 3,
        scratch_shapes=[dma((3,))],
        cost_estimate=pl.CostEstimate(flops=10**7, bytes_accessed=8 * 10**6, transcendentals=0),
        compiler_params=pltpu.CompilerParams(vmem_limit_bytes=8 << 20),
        name="put",
    )(*results)


def fits(queries, store, owners):
    n, tp = lax.axis_size("st"), lax.axis_size("tp")
    blocks = owners.shape[0]
    block_len = queries.shape[0] // blocks
    slot_cap = (2 * owners.size + n - 1) // n
    return (
        n % 2 == 0 and n >= 8 and tp == 4 and blocks == 8 and n * blocks <= 128
        and block_len == 128 and queries.shape[1] == 2 * HD
        and store.shape[0] % (tp * CHUNK // 2) == 0 and store.shape[0] % 256 == 0
        and store.shape[0] // PLEN <= 128 and store.shape[1] % (256 * n) == 0
        and 8 * slot_cap * PLEN >= 3 * queries.shape[0]
    )


def local(*arrays):
    if fits(arrays[0], arrays[3], arrays[7]):
        return query_plan(*arrays)
    return passage_plan(*arrays)


def solution(mesh):
    placed = (
        P("st", "tp"),
        P("st", "tp"),
        P("st", "tp"),
        P("st", None),
        P(),
        P(None, "tp"),
        P(None, "tp"),
        P("st", None),
        P("st", None),
    )
    return jax.shard_map(
        local,
        mesh=mesh,
        in_specs=placed,
        out_specs=(P("st", "tp"), P(("st", "tp"), None), P("st", "tp")),
        check_vma=False,
    )
```
